32 devices in a mesh: ep: 8 (over z, x), tp: 4 (over y, core).
Axes of the slice: x: 2, y: 2, z: 4, core: 2. Of those that a mesh axis runs over, the one named last changes fastest.
Arguments:
- queries: bfloat16 [8192, 2048], P('ep', 'tp'), may hold values from -128 to 128
- key_heads: bfloat16 [8192, 1024], P('ep', 'tp'), may hold values from -6 to 6
- value_heads: bfloat16 [8192, 1024], P('ep', 'tp'), may hold values from -6 to 6
- sink_logits: float32 [32], P('tp'), may hold values from 1 to 5
- mix_weight: bfloat16 [2048, 2048], replicated, may hold values from -1 to 1
- expert_input: bfloat16 [4096, 2048], P(('ep', 'tp')), may hold values from -6 to 6
- norm_gain: float32 [2048], replicated, may hold values from 0.1 to 1.9
- routes: int32 [4096, 4], P(('ep', 'tp')), may hold values from 0 to 31, all different within a row; in each aligned block of 128 rows (0 to 127, 128 to 255, ...) at most 32 rows name the same one
- route_weights: float32 [4096, 4], P(('ep', 'tp')), may hold values from 0.1 to 1
- gate_weight: bfloat16 [32, 2048, 1024], P(('ep', 'tp')), may hold values from -0.375 to 0.375
- up_weight: bfloat16 [32, 2048, 1024], P(('ep', 'tp')), may hold values from -0.375 to 0.375
- down_weight: bfloat16 [32, 1024, 2048], P(('ep', 'tp')), may hold values from -0.046875 to 0.046875
Outputs:
- mixer_out: bfloat16 [8192, 2048], P(('ep', 'tp'))
- experts_out: bfloat16 [4096, 2048], P(('ep', 'tp'))
The draws below stay inside these ranges and needn't reach their ends.
Inputs may be any that keep to these rules, and one draw needn't show every extreme that they name: `routes`: each row names 4 different experts; within the 128 rows of one device no expert is named more than 32 times, and in some devices' rows some expert is named exactly 32 times.
All inputs are finite; a program needn't handle non-finite values.
Results may differ from the reference program's by a relative error of at most 0.012.
The reference program's roundings to bfloat16 on the way count: a program that leaves them out, or rounds other values in their place, can miss the bound.
Values may be sent and summed in bfloat16 or wider, within the bound.
No kernel may reach another device: no remote copies, remote signals or barrier semaphores. Data moves between devices by JAX's collectives and lax.ppermute only.
A program may use at most 128 MiB of HBM per device.

```python
import math
import jax
import jax.numpy as jnp
import numpy as np
from jax import lax

D = 2048
HEADS = 32
KV_HEADS = 16
HEAD_DIM = 64
WINDOW = 128
GRID_W = 64
FF = 1024
TOPK = 4
TOK_B = 128
TOKENS_A = 8192
TOKENS_B = 4096
EXPERTS = 32
CAP = 32
N_EP = 8
N_TP = 4


def query_key_pair(key):
    base_seed = jax.random.fold_in(key, 7)
    query_seed, key_seed = jax.random.split(base_seed, 2)
    length = TOKENS_A
    key_part = jnp.clip(jax.random.normal(key_seed, (length, KV_HEADS * HEAD_DIM), jnp.float32), -4.0, 4.0)
    query_part = jnp.clip(jax.random.normal(query_seed, (length, HEADS * HEAD_DIM), jnp.float32), -4.0, 4.0)
    return (query_part, key_part)


def draw_queries(key, part):
    return query_key_pair(key)[0].astype(jnp.bfloat16)


def draw_key_heads(key, part):
    return query_key_pair(key)[1].astype(jnp.bfloat16)


def level_of(own_key, extent, pieces, least, top_value):
    gain = 1.0
    for position, blocks in pieces:
        draws = jax.random.uniform(jax.random.fold_in(jax.random.fold_in(own_key, 6), position), (blocks,), jnp.float32, least / len(pieces), top_value / len(pieces))
        gain = gain * jnp.repeat(jnp.exp(draws), extent[position] // blocks).reshape((-1,) + (1,) * (len(extent) - 1 - position))
    return gain


def routed_block(stream_key, own, number, rows, number_of, top, bound, slope):
    sequence = jax.random.permutation(stream_key, number_of)
    heavy_load, usual = shares(number_of, rows * top, bound, slope, True), shares(number_of, rows * top, bound, slope, False)
    places = jnp.arange(number_of)

    def named(lengths, turn):
        used = int((lengths > 0).sum())
        fixed = max(1, used // 4)
        shifted = fixed + (places - fixed + turn * (used - fixed)) % max(1, number_of - fixed)
        return jnp.zeros((number_of,), jnp.int32).at[sequence[jnp.where(places < fixed, places, shifted)]].set(jnp.asarray(lengths, jnp.int32))

    lengths = jnp.where(number % 4 == 0, named(heavy_load, number // 4), named(usual, number - number // 4 - 1))
    mixed = jax.random.permutation(jax.random.fold_in(own, 3), number_of)
    giver, taker = mixed[0:number_of // 2 * 2:2], mixed[1:number_of // 2 * 2:2]
    room = jnp.minimum(lengths[giver] - 1, bound - lengths[taker]) // 2
    room = jnp.where((giver == sequence[0]) | (taker == sequence[0]) | (lengths[taker] == 0), 0, jnp.maximum(room, 0))
    shifted = jax.random.randint(jax.random.fold_in(own, 4), (number_of // 2,), 0, 1 << 20) % (room + 1)
    lengths = lengths.at[giver].add(-shifted).at[taker].add(shifted)
    items = jnp.searchsorted(jnp.cumsum(lengths), jnp.arange(rows * top), side="right").astype(jnp.int32)
    table = items.reshape(top, rows).T
    table = table[jax.random.permutation(jax.random.fold_in(own, 1), rows)]
    turn = jax.random.randint(jax.random.fold_in(own, 2), (rows, 1), 0, top)
    return jnp.take_along_axis(table, (jnp.arange(top)[None, :] + turn) % top, axis=1)


def shares(count, total, most, skew, full):
    loads = [(1 << 20) // math.isqrt(rank ** skew) + 1 for rank in range(1, count + 1)]
    largest = most if full else min(most, max(-(-total // count), total * loads[0] // sum(loads)))
    least = 1 if total - largest >= count - 1 else 0
    counts, rest = [largest] + [least] * (count - 1), total - largest - least * (count - 1)
    while rest > 0:
        candidates = [i for i in range(1, count) if counts[i] < largest] or [i for i in range(1, count) if counts[i] < most]
        whole, budget = sum([loads[i] for i in candidates]), rest
        for i in candidates:
            extra = min(most - counts[i], max(1, budget * loads[i] // whole), rest)
            counts[i] = counts[i] + extra
            rest = rest - extra
    return np.array(counts)


def scatter_about(key, extent, scale, reach, shards=(), kind=jnp.bfloat16):
    result = scale * jax.random.normal(key, extent, jnp.float32)
    if shards:
        result = result * level_of(key, extent, shards, -0.22, 0.18)
    return jnp.clip(result, -reach, reach).astype(kind)


def setup_inputs(seed: int = 0) -> dict:
    key_list = jax.random.split(jax.random.key(seed), 13)
    queries = draw_queries(jax.random.fold_in(key_list[12], 71), 0)
    key_heads = draw_key_heads(jax.random.fold_in(key_list[12], 71), 0)
    value_heads = scatter_about(key_list[2], (TOKENS_A, KV_HEADS * HEAD_DIM), 1.0, 6.0, ((0, 8), (1, 4)))
    sink_logits = jnp.clip(1.0 + 4.0 * jax.random.uniform(key_list[3], (HEADS,), jnp.float32) ** level_of(key_list[3], (HEADS,), ((0, 4),), -0.2, 0.2), 1.0, 5.0)
    mix_weight = scatter_about(key_list[4], (HEADS * HEAD_DIM, D), (HEADS * HEAD_DIM // 64) ** -0.5, 1.0)
    expert_input = scatter_about(key_list[5], (TOKENS_B, D), 1.0, 6.0, ((0, 32),))
    norm_gain = jnp.clip(1.0 + 0.18 * jax.random.normal(key_list[6], (D,), jnp.float32), 0.1, 1.9)
    routes_keys = jax.random.split(jax.random.fold_in(key_list[7], 1), TOKENS_B // TOK_B)
    routes_turns = jax.random.permutation(jax.random.fold_in(key_list[7], 3), TOKENS_B // TOK_B)
    routes = jax.vmap(lambda own, number: routed_block(jax.random.fold_in(key_list[7], 2), own, number, TOK_B, EXPERTS, TOPK, CAP, 2))(routes_keys, routes_turns).reshape((TOKENS_B, TOPK))
    route_weights = jnp.clip(jnp.exp(math.log(1.0) - 2.3025851 * jax.random.uniform(key_list[8], (TOKENS_B, TOPK), jnp.float32) ** level_of(key_list[8], (TOKENS_B, TOPK), ((0, 32),), -0.2, 0.2)), 0.1, 1.0)
    gate_weight = scatter_about(key_list[9], (EXPERTS, D, FF), (D // 9) ** -0.5, 0.375, ((0, 32),))
    up_weight = scatter_about(key_list[10], (EXPERTS, D, FF), (D // 9) ** -0.5, 0.375, ((0, 32),))
    down_weight = scatter_about(key_list[11], (EXPERTS, FF, D), (FF * 16) ** -0.5, 0.046875, ((0, 32),))
    return {"queries": queries, "key_heads": key_heads, "value_heads": value_heads, "sink_logits": sink_logits, "mix_weight": mix_weight, "expert_input": expert_input, "norm_gain": norm_gain, "routes": routes, "route_weights": route_weights, "gate_weight": gate_weight, "up_weight": up_weight, "down_weight": down_weight}


ROPE_BASE = 10000.0
CLAMP_LIMIT = 7.0
GATE_SLOPE = 1.702
NORM_EPS = 1e-05

def rotate_pairs(table, grid_rows, grid_cols, head_width):
    length = table.shape[0]
    quarter = head_width // 4
    shaped = table.reshape(length, -1, 2, 2, quarter)
    freqs = ROPE_BASE ** (-jnp.arange(0, head_width // 2, 2, dtype=jnp.float32) / (head_width // 2))
    angles = jnp.stack([grid_rows, grid_cols], axis=-1)[:, :, None] * freqs
    cosines = jnp.cos(angles)[:, None]
    sine_part = jnp.sin(angles)[:, None]
    former = shaped[..., 0, :]
    latter = shaped[..., 1, :]
    turned = jnp.stack([former * cosines - latter * sine_part, latter * cosines + former * sine_part], axis=-2)
    return turned.reshape(length, -1)

def grid_place(positions):
    return ((positions // GRID_W).astype(jnp.float32), (positions % GRID_W).astype(jnp.float32))

def attend(queries, key_heads, value_heads, sink_logits):
    length = queries.shape[0]
    group_size = HEADS // KV_HEADS
    positions = jnp.arange(length, dtype=jnp.int32)
    grid_rows, grid_cols = grid_place(positions)
    q_rot = rotate_pairs(queries.astype(jnp.float32), grid_rows, grid_cols, HEAD_DIM).astype(jnp.bfloat16)
    k_rot = rotate_pairs(key_heads.astype(jnp.float32), grid_rows, grid_cols, HEAD_DIM).astype(jnp.bfloat16)
    k_padded = jnp.pad(k_rot, ((WINDOW, WINDOW), (0, 0)))
    v_padded = jnp.pad(value_heads, ((WINDOW, WINDOW), (0, 0)))
    block_rows = math.gcd(length, 512)
    key_span = block_rows + 2 * WINDOW
    sink_grid = sink_logits.astype(jnp.float32).reshape(KV_HEADS, group_size)

    def one_block(block_index):
        first_row = block_index * block_rows
        q_blk = lax.dynamic_slice_in_dim(q_rot, first_row, block_rows, 0).astype(jnp.float32)
        q_blk = q_blk.reshape(block_rows, KV_HEADS, group_size, HEAD_DIM)
        k_blk = lax.dynamic_slice_in_dim(k_padded, first_row, key_span, 0).astype(jnp.float32)
        k_blk = k_blk.reshape(key_span, KV_HEADS, HEAD_DIM)
        v_blk = lax.dynamic_slice_in_dim(v_padded, first_row, key_span, 0).astype(jnp.float32)
        v_blk = v_blk.reshape(key_span, KV_HEADS, HEAD_DIM)
        q_pos = first_row + jnp.arange(block_rows, dtype=jnp.int32)
        k_pos = first_row - WINDOW + jnp.arange(key_span, dtype=jnp.int32)
        inside = (jnp.abs(q_pos[:, None] - k_pos[None, :]) <= WINDOW) & (k_pos >= 0) & (k_pos < length)
        scores = jnp.einsum('qkgd,skd->kgqs', q_blk, k_blk) * HEAD_DIM ** (-0.5)
        scores = jnp.where(inside, scores, -jnp.inf)
        peak = jnp.maximum(lax.optimization_barrier(jnp.max(scores, axis=-1)), sink_grid[:, :, None])
        weights_exp = jnp.exp(scores - peak[..., None])
        denominator = lax.optimization_barrier(jnp.sum(weights_exp, axis=-1)) + jnp.exp(sink_grid[:, :, None] - peak)
        chances = (weights_exp / denominator[..., None]).astype(jnp.bfloat16)
        blended = jnp.einsum('kgqs,skd->qkgd', chances.astype(jnp.float32), v_blk)
        return blended.astype(jnp.bfloat16).reshape(block_rows, HEADS * HEAD_DIM)
    blocks = lax.map(one_block, jnp.arange(length // block_rows, dtype=jnp.int32))
    return blocks.reshape(length, HEADS * HEAD_DIM)

def normalize(tokens_in, gain_row):
    values = tokens_in.astype(jnp.float32)
    center = lax.optimization_barrier(jnp.mean(values, axis=-1, keepdims=True))
    spread = lax.optimization_barrier(jnp.mean(jnp.square(values - center), axis=-1, keepdims=True))
    return ((values - center) * lax.rsqrt(spread + NORM_EPS) * gain_row.astype(jnp.float32)).astype(jnp.bfloat16)

def expert_rows(row_block, w_gate, w_lift, w_down):
    gate_pre = jnp.dot(row_block, w_gate, preferred_element_type=jnp.float32)
    lift_pre = jnp.dot(row_block, w_lift, preferred_element_type=jnp.float32)
    gate_pre = jnp.minimum(gate_pre, CLAMP_LIMIT)
    lift_pre = jnp.clip(lift_pre, -CLAMP_LIMIT, CLAMP_LIMIT)
    activated = ((lift_pre + 1.0) * gate_pre * jax.nn.sigmoid(GATE_SLOPE * gate_pre)).astype(jnp.bfloat16)
    return jnp.dot(activated, w_down, preferred_element_type=jnp.float32).astype(jnp.bfloat16)

def slot_within(route_block):
    flat_routes = route_block.reshape(-1)
    matches = (flat_routes[:, None] == jnp.arange(EXPERTS, dtype=jnp.int32)[None, :]).astype(jnp.int32)
    earlier = jnp.cumsum(matches, axis=0) - matches
    return lax.optimization_barrier(jnp.sum(earlier * matches, axis=1)).astype(jnp.int32)

def reference(queries, key_heads, value_heads, sink_logits, mix_weight, expert_input, norm_gain, routes, route_weights, gate_weight, up_weight, down_weight):
    attended = attend(queries, key_heads, value_heads, sink_logits)
    mixer_out = jnp.dot(attended, mix_weight, preferred_element_type=jnp.float32).astype(jnp.bfloat16)
    sources = N_EP * N_TP
    normed = normalize(expert_input, norm_gain)
    slots = jax.vmap(slot_within)(routes.reshape(sources, TOK_B, TOPK)).reshape(-1)
    flat_routes = routes.reshape(-1).astype(jnp.int32)
    token_of = (jnp.arange(TOKENS_B * TOPK, dtype=jnp.int32) // TOPK).astype(jnp.int32)
    source_of = (token_of // TOK_B).astype(jnp.int32)
    columns = (source_of * CAP + slots).astype(jnp.int32)
    table = jnp.full((EXPERTS, sources * CAP), TOKENS_B, jnp.int32).at[flat_routes, columns].set(token_of)
    padded_in = jnp.concatenate([normed, jnp.zeros((1, D), jnp.bfloat16)], axis=0)

    def one_expert(bundle):
        row_ids, w_gate, w_lift, w_down = bundle
        return expert_rows(padded_in[row_ids], w_gate, w_lift, w_down)
    results = lax.map(one_expert, (table, gate_weight, up_weight, down_weight))
    picked = results[flat_routes, columns].reshape(TOKENS_B, TOPK, D)
    summed = lax.optimization_barrier(jnp.sum(route_weights.astype(jnp.float32)[..., None] * picked.astype(jnp.float32), axis=1))
    return (mixer_out, summed.astype(jnp.bfloat16))
```

```python
import functools
import math

import jax
import jax.numpy as jnp
from jax import lax
from jax.experimental import pallas as pl
from jax.experimental.pallas import tpu as pltpu
from jax.sharding import Mesh
from jax.sharding import PartitionSpec as P

HEAD_DIM = 64
WINDOW = 128
GRID_W = 64
ROPE_BASE = 10000.0
CLAMP_LIMIT = 7.0
GATE_SLOPE = 1.702
NORM_EPS = 1e-05
LANES = 128
MASKED = -1e30

VMEM = pl.BlockSpec(memory_space=pltpu.VMEM)
SMEM = pl.BlockSpec(memory_space=pltpu.SMEM)
BF16 = jnp.bfloat16
F32 = jnp.float32


def iota(shape, dim):
    return lax.broadcasted_iota(jnp.int32, shape, dim)


def norm_kernel(x_ref, gain_ref, extra_ref, out_ref):
    width = x_ref.shape[1]
    values = x_ref[...].astype(F32)
    center = jnp.mean(values, axis=-1, keepdims=True)
    shifted = values - center
    spread = jnp.mean(jnp.square(shifted), axis=-1, keepdims=True)
    normed = shifted * lax.rsqrt(spread + NORM_EPS) * gain_ref[...]
    out_ref[:, :width] = normed.astype(BF16)
    out_ref[:, width:] = extra_ref[...]


def make_payload(x, gain, routes, weights):
    tokens, width = x.shape
    top = routes.shape[1]
    high = weights.astype(BF16)
    low = (weights - high.astype(F32)).astype(BF16)
    fill = jnp.zeros((tokens, LANES - 3 * top), BF16)
    extra = jnp.concatenate([routes.astype(BF16), high, low, fill], axis=1)
    return pl.pallas_call(
        norm_kernel,
        out_shape=jax.ShapeDtypeStruct((tokens, width + LANES), BF16),
        in_specs=[VMEM, VMEM, VMEM],
        out_specs=VMEM,
        name="norm",
    )(x, gain.reshape(1, width), extra)


def slot_match(extra, where_ref, plan, weighted):
    tokens = extra.shape[0]
    top, cap, plane, xor = plan
    lane = iota((1, LANES), 1)
    piece = lane ^ where_ref[1] if xor else lane
    target = jnp.where(lane < plane, where_ref[0] + piece, -1).astype(F32)
    named = jnp.zeros((tokens, LANES), F32)
    high = jnp.zeros((tokens, LANES), F32)
    low = jnp.zeros((tokens, LANES), F32)
    for k in range(top):
        hit = extra[:, k : k + 1] == target
        named = jnp.where(hit, 1.0, named)
        if weighted:
            high = jnp.where(hit, extra[:, top + k : top + k + 1], high)
            low = jnp.where(hit, extra[:, 2 * top + k : 2 * top + k + 1], low)
    earlier = (iota((tokens, tokens), 1) < iota((tokens, tokens), 0)).astype(F32).astype(BF16)
    slot = jnp.dot(earlier, named.astype(BF16), preferred_element_type=F32)
    slot = jnp.where(named > 0.5, slot, -1.0)
    columns = plane * cap
    spread = (iota((LANES, columns), 1) // cap == iota((LANES, columns), 0)).astype(F32).astype(BF16)
    place = (iota((1, columns), 1) % cap).astype(F32)
    slot = jnp.dot(slot.astype(BF16), spread, preferred_element_type=F32)
    match = slot == place
    if not weighted:
        return jnp.where(match, 1.0, 0.0)
    high = jnp.dot(high.astype(BF16), spread, preferred_element_type=F32)
    low = jnp.dot(low.astype(BF16), spread, preferred_element_type=F32)
    zero = jnp.zeros_like(high)
    return jnp.where(match, high, zero).astype(BF16), jnp.where(match, low, zero).astype(BF16)


def dispatch_kernel(plan, pieces, where_ref, payload_ref, *out_refs):
    width = payload_ref.shape[1] - LANES
    extra = payload_ref[:, width:].astype(F32)
    match = slot_match(extra, where_ref, plan, False)
    turned = jnp.transpose(match).astype(BF16)
    rows = turned.shape[0] // pieces
    step = math.gcd(width, 512)
    for left in range(0, width, step):
        block = jnp.dot(turned, payload_ref[:, left : left + step], preferred_element_type=F32)
        block = block.astype(BF16)
        for i in range(pieces):
            out_refs[i][:, left : left + step] = block[i * rows : (i + 1) * rows]


def dispatch(plan, pieces, where, payload):
    width = payload.shape[1] - LANES
    rows = plan[1] * plan[2] // pieces
    return pl.pallas_call(
        functools.partial(dispatch_kernel, plan, pieces),
        out_shape=[jax.ShapeDtypeStruct((rows, width), BF16)] * pieces,
        in_specs=[SMEM, VMEM],
        out_specs=[VMEM] * pieces,
        name="dispatch",
    )(where, payload)


def combine_kernel(plan, pieces, adds, where_ref, extra_ref, *refs):
    back_refs, add_refs, out_ref = refs[:pieces], refs[pieces : pieces + adds], refs[-1]
    width = out_ref.shape[1]
    high, low = slot_match(extra_ref[...].astype(F32), where_ref, plan, True)
    step = math.gcd(width, 512)
    for left in range(0, width, step):
        cut = slice(left, left + step)
        rows = jnp.concatenate([r[:, cut] for r in back_refs], axis=0)
        total = jnp.dot(high, rows, preferred_element_type=F32)
        total = total + jnp.dot(low, rows, preferred_element_type=F32)
        for r in add_refs:
            total = total + r[:, cut].astype(F32)
        out_ref[:, cut] = total.astype(BF16)


def combine(plan, where, payload, back, adds):
    tokens, wide = payload.shape
    width = wide - LANES
    edge = pl.BlockSpec((tokens, LANES), lambda i: (0, width // LANES))
    return pl.pallas_call(
        functools.partial(combine_kernel, plan, len(back), len(adds)),
        grid=(1,),
        out_shape=jax.ShapeDtypeStruct((tokens, width), BF16),
        in_specs=[SMEM, edge] + [VMEM] * (len(back) + len(adds)),
        out_specs=VMEM,
        name="combine",
    )(where, payload, *back, *adds)


def expert_kernel(pieces, steps, gate_ref, up_ref, down_ref, *refs):
    in_refs, out_refs = refs[:pieces], refs[pieces : 2 * pieces]
    x_ref, act_ref = refs[2 * pieces :]
    rows = in_refs[0].shape[0]
    tile = gate_ref.shape[2]
    index = pl.program_id(0)

    @pl.when(index == 0)
    def _():
        for i in range(pieces):
            x_ref[i * rows : (i + 1) * rows, :] = in_refs[i][...]

    for s in range(steps):

        @pl.when(index == s)
        def _():
            x = x_ref[...]
            gate = jnp.dot(x, gate_ref[0], preferred_element_type=F32)
            lift = jnp.dot(x, up_ref[0], preferred_element_type=F32)
            gate = jnp.minimum(gate, CLAMP_LIMIT)
            lift = jnp.clip(lift, -CLAMP_LIMIT, CLAMP_LIMIT)
            act = (lift + 1.0) * gate * jax.nn.sigmoid(GATE_SLOPE * gate)
            act_ref[:, s * tile : (s + 1) * tile] = act.astype(BF16)

    @pl.when(index >= steps)
    def _():
        done = jnp.dot(act_ref[...], down_ref[0], preferred_element_type=F32).astype(BF16)
        for i in range(pieces):
            out_refs[i][...] = done[i * rows : (i + 1) * rows]


def experts(parts, w_gate, w_up, w_down):
    pieces = len(parts)
    rows, width = parts[0].shape
    hidden = w_gate.shape[2]
    tile = math.gcd(hidden, 256)
    steps = hidden // tile
    wide = math.gcd(width, 512)
    blocks = width // wide
    first = lambda i: (0, 0, jnp.minimum(i, steps - 1))
    second = lambda i: (0, 0, jnp.maximum(i - steps, 0))
    flops = 6 * pieces * rows * width * hidden
    return pl.pallas_call(
        functools.partial(expert_kernel, pieces, steps),
        grid=(steps + blocks,),
        in_specs=[
            pl.BlockSpec((1, width, tile), first),
            pl.BlockSpec((1, width, tile), first),
            pl.BlockSpec((1, hidden, wide), second),
        ]
        + [VMEM] * pieces,
        out_specs=[pl.BlockSpec((rows, wide), lambda i: (0, jnp.maximum(i - steps, 0)))] * pieces,
        out_shape=[jax.ShapeDtypeStruct((rows, width), BF16)] * pieces,
        scratch_shapes=[
            pltpu.VMEM((pieces * rows, width), BF16),
            pltpu.VMEM((pieces * rows, hidden), BF16),
        ],
        cost_estimate=pl.CostEstimate(
            flops=flops, transcendentals=0, bytes_accessed=6 * width * hidden
        ),
        name="experts",
    )(w_gate, w_up, w_down, *parts)


def rope_block(x, cos, sin):
    lane = iota((1, LANES), 1)
    quarter = HEAD_DIM // 4
    ahead = pltpu.roll(x, LANES - quarter, axis=1)
    behind = pltpu.roll(x, quarter, axis=1)
    mate = jnp.where(lane % (2 * quarter) < quarter, ahead, behind)
    return x * cos + mate * sin


def attention_kernel(
    q_block, info_ref, sink_ref, table_ref, q_ref, k_ref, v_ref, left_ref, right_ref, out_ref,
    k_all, v_all, band_ref,
):
    rows = q_ref.shape[0]
    kv_width = k_ref.shape[1]
    pairs = kv_width // LANES
    group = q_ref.shape[1] // kv_width
    span = q_block + 2 * WINDOW
    grid_rows = (rows + 2 * WINDOW) // GRID_W
    lane = iota((1, LANES), 1)
    by_row = lane % HEAD_DIM < HEAD_DIM // 2
    half = lane < HEAD_DIM
    cols = grid_rows
    total = grid_rows + GRID_W
    col_cos = table_ref[cols : cols + GRID_W, :]
    col_sin = table_ref[total + cols : total + cols + GRID_W, :]

    def tables(first, count):
        cos, sin = [], []
        for i in range(count // GRID_W):
            r = first + i
            cos.append(jnp.where(by_row, table_ref[pl.ds(r, 1), :], col_cos))
            sin.append(jnp.where(by_row, table_ref[pl.ds(total + r, 1), :], col_sin))
        return jnp.concatenate(cos, axis=0), jnp.concatenate(sin, axis=0)

    def turn_keys(source, source_row, target_row, count, grid_row):
        cos, sin = tables(grid_row, count)
        for p in range(pairs):
            part = source[pl.ds(source_row, count), p * LANES : (p + 1) * LANES].astype(F32)
            k_all[pl.ds(target_row, count), p * LANES : (p + 1) * LANES] = rope_block(
                part, cos, sin
            ).astype(BF16)

    turn_keys(left_ref, 0, 0, WINDOW, 0)
    turn_keys(right_ref, 0, rows + WINDOW, WINDOW, (rows + WINDOW) // GRID_W)

    def keys_step(b, carry):
        at = pl.multiple_of(b * WINDOW, WINDOW)
        turn_keys(k_ref, at, at + WINDOW, WINDOW, (b + 1) * (WINDOW // GRID_W))
        return carry

    lax.fori_loop(0, rows // WINDOW, keys_step, 0)
    v_all[0:WINDOW, :] = left_ref[:, kv_width:]
    v_all[WINDOW : WINDOW + rows, :] = v_ref[...]
    v_all[WINDOW + rows :, :] = right_ref[:, kv_width:]
    gap = iota((q_block, span), 1) - iota((q_block, span), 0)
    band_ref[...] = jnp.where((gap >= 0) & (gap <= 2 * WINDOW), 0.0, MASKED)

    def block_step(b, carry):
        at = pl.multiple_of(b * q_block, q_block)
        cos, sin = tables(b * (q_block // GRID_W) + WINDOW // GRID_W, q_block)
        place = info_ref[0] + at - WINDOW + iota((1, span), 1)
        bias = band_ref[...] + jnp.where((place >= 0) & (place < info_ref[1]), 0.0, MASKED)
        for p in range(pairs):
            heads = []
            for c in range(group):
                left = (p * group + c) * LANES
                x = q_ref[pl.ds(at, q_block), left : left + LANES].astype(F32)
                x = rope_block(x, cos, sin).astype(BF16).astype(F32) * HEAD_DIM**-0.5
                swapped = pltpu.roll(x, HEAD_DIM, axis=1)
                low_side = c < group // 2
                for one in (x, swapped) if low_side else (swapped, x):
                    keep = half if low_side else jnp.logical_not(half)
                    heads.append(jnp.where(keep, one, 0.0).astype(BF16))
            keys = k_all[pl.ds(at, span), p * LANES : (p + 1) * LANES]
            values = v_all[pl.ds(at, span), p * LANES : (p + 1) * LANES]
            done = []
            for h in range(2 * group):
                scores = lax.dot_general(
                    heads[h], keys, (((1,), (1,)), ((), ())), preferred_element_type=F32
                )
                scores = scores + bias
                sink = sink_ref[p * 2 * group + h]
                peak = jnp.maximum(jnp.max(scores, axis=-1, keepdims=True), sink)
                exps = jnp.exp(scores - peak)
                bottom = jnp.sum(exps, axis=-1, keepdims=True) + jnp.exp(sink - peak)
                chances = (exps * (1.0 / bottom)).astype(BF16)
                done.append(jnp.dot(chances, values, preferred_element_type=F32))
            for c in range(group):
                one, two = done[2 * c], done[2 * c + 1]
                if c < group // 2:
                    two = pltpu.roll(two, HEAD_DIM, axis=1)
                else:
                    one = pltpu.roll(one, HEAD_DIM, axis=1)
                left = (p * group + c) * LANES
                out_ref[pl.ds(at, q_block), left : left + LANES] = jnp.where(
                    half, one, two
                ).astype(BF16)
        return carry

    lax.fori_loop(0, rows // q_block, block_step, 0)


def attention(q, k, v, left, right, sink, first_global, length):
    rows = q.shape[0]
    kv_width = k.shape[1]
    group = q.shape[1] // kv_width
    assert kv_width % LANES == 0 and group == 2 and rows % WINDOW == 0
    assert rows % GRID_W == 0 and WINDOW % GRID_W == 0
    q_block = WINDOW
    span = q_block + 2 * WINDOW
    grid_rows = (rows + 2 * WINDOW) // GRID_W
    quarter = HEAD_DIM // 4
    freqs = ROPE_BASE ** (-jnp.arange(0, HEAD_DIM // 2, 2, dtype=F32) / (HEAD_DIM // 2))
    lane_freq = jnp.tile(freqs, LANES // quarter)
    row_at = (first_global - WINDOW) // GRID_W + jnp.arange(grid_rows, dtype=jnp.int32)
    spots = jnp.concatenate([row_at, jnp.arange(GRID_W, dtype=jnp.int32)]).astype(F32)
    angles = spots[:, None] * lane_freq[None, :]
    sign = jnp.where(jnp.arange(LANES) % (2 * quarter) < quarter, -1.0, 1.0)
    table = jnp.concatenate([jnp.cos(angles), jnp.sin(angles) * sign[None, :]], axis=0)
    info = jnp.stack([first_global, jnp.int32(length)]).astype(jnp.int32)
    heads = q.shape[1] // HEAD_DIM
    return pl.pallas_call(
        functools.partial(attention_kernel, q_block),
        out_shape=jax.ShapeDtypeStruct(q.shape, BF16),
        in_specs=[SMEM, SMEM] + [VMEM] * 6,
        out_specs=VMEM,
        scratch_shapes=[
            pltpu.VMEM((rows + 2 * WINDOW, kv_width), BF16),
            pltpu.VMEM((rows + 2 * WINDOW, kv_width), BF16),
            pltpu.VMEM((q_block, span), F32),
        ],
        cost_estimate=pl.CostEstimate(
            flops=4 * rows * span * heads * HEAD_DIM * 6,
            transcendentals=rows * span * heads,
            bytes_accessed=8 * rows * kv_width * 2,
        ),
        name="attention",
    )(info, sink, table, q, k, v, left, right)


def relay(x, axis):
    return lax.ppermute(x, axis, [(0, 1), (1, 0)])


def body(
    queries,
    key_heads,
    value_heads,
    sink_logits,
    mix_weight,
    expert_input,
    norm_gain,
    routes,
    route_weights,
    gate_weight,
    up_weight,
    down_weight,
):
    ring = ("zh", "zl", "xx")
    inner = ("xx", "tp")
    ring_size = lax.axis_size(ring)
    tp_size = lax.axis_size("tp")
    plane = lax.axis_size(inner)
    experts_all = ring_size * tp_size
    tok_local, top = routes.shape
    cap = 2 * tok_local * top // experts_all
    xor = plane <= 8 and plane & (plane - 1) == 0
    pieces = plane if xor else 1
    plan = (top, cap, plane, xor)
    position = lax.axis_index(inner)
    base = lax.axis_index(("zh", "zl")) * plane
    where = jnp.stack([base, position]).astype(jnp.int32)

    def exchange(parts):
        if not xor:
            block = parts[0].reshape(plane, cap, -1)
            return [lax.all_to_all(block, inner, 0, 0, tiled=True).reshape(parts[0].shape)]
        return [parts[0]] + [
            lax.ppermute(parts[p], inner, [(i, i ^ p) for i in range(plane)])
            for p in range(1, plane)
        ]

    own = make_payload(expert_input, norm_gain, routes, route_weights)
    near = relay(own, "zl")
    far = relay(own, "zh")
    far_near = relay(far, "zl")
    chunks = (own, near, far, far_near)
    arrived = [exchange(dispatch(plan, pieces, where, chunk)) for chunk in chunks]

    rows_here = queries.shape[0]
    first_global = lax.axis_index(ring) * rows_here
    tail = jnp.concatenate([key_heads[-WINDOW:], value_heads[-WINDOW:]], axis=1)
    head = jnp.concatenate([key_heads[:WINDOW], value_heads[:WINDOW]], axis=1)
    ends = ring_size - 1
    left = lax.ppermute(tail, ring, [(i, i + 1) for i in range(ends)])
    right = lax.ppermute(head, ring, [(i + 1, i) for i in range(ends)])
    attended = attention(
        queries, key_heads, value_heads, left, right, sink_logits,
        first_global, rows_here * ring_size,
    )
    token_rows = lax.all_to_all(attended, "tp", split_axis=0, concat_axis=1, tiled=True)
    mixer_out = jnp.dot(token_rows, mix_weight, preferred_element_type=F32).astype(BF16)

    made = [experts(parts, gate_weight, up_weight, down_weight) for parts in arrived]
    back = [exchange(made[i]) for i in (3, 2, 1, 0)][::-1]
    last = combine(plan, where, far_near, back[3], [])
    mid = combine(plan, where, far, back[2], [relay(last, "zl")])
    side = combine(plan, where, near, back[1], [])
    summed = combine(plan, where, own, back[0], [relay(side, "zl"), relay(mid, "zh")])
    return (mixer_out, summed)


def solution(mesh):
    n_ep, n_tp = mesh.shape["ep"], mesh.shape["tp"]
    assert n_ep % 4 == 0
    fine = Mesh(mesh.devices.reshape(2, 2, n_ep // 4, n_tp), ("zh", "zl", "xx", "tp"))
    ring = ("zh", "zl", "xx")
    every = ring + ("tp",)
    return jax.shard_map(
        body,
        mesh=fine,
        in_specs=(
            P(ring, "tp"),
            P(ring, "tp"),
            P(ring, "tp"),
            P("tp"),
            P(),
            P(every, None),
            P(),
            P(every, None),
            P(every, None),
            P(every, None, None),
            P(every, None, None),
            P(every, None, None),
        ),
        out_specs=(P(every, None), P(every, None)),
        check_vma=False,
    )
```

```python
import functools
import math

import jax
import jax.numpy as jnp
from jax import lax
from jax.experimental import pallas as pl
from jax.experimental.pallas import tpu as pltpu
from jax.sharding import Mesh
from jax.sharding import PartitionSpec as P


HEAD_DIM = 64
WINDOW = 128
GRID_W = 64
ROPE_BASE = 10000.0
CLAMP_LIMIT = 7.0
GATE_SLOPE = 1.702
NORM_EPS = 1e-05
LANES = 128
MASKED = -1e30

VMEM = pl.BlockSpec(memory_space=pltpu.VMEM)
SMEM = pl.BlockSpec(memory_space=pltpu.SMEM)
ANY = pl.BlockSpec(memory_space=pl.ANY)
HBM = pl.BlockSpec(memory_space=pltpu.HBM)
BF16 = jnp.bfloat16
F32 = jnp.float32


def cost(flops):
    return pl.CostEstimate(flops=int(flops), transcendentals=0, bytes_accessed=1 << 20)


def params(mebibytes):
    return pltpu.CompilerParams(vmem_limit_bytes=mebibytes << 20)


def iota(shape, dim):
    return lax.broadcasted_iota(jnp.int32, shape, dim)


def fetch(pairs, sems):
    copies = [pltpu.make_async_copy(s, t, sems.at[i]) for i, (s, t) in enumerate(pairs)]
    for copy in copies:
        copy.start()
    for copy in copies:
        copy.wait()


def norm_kernel(x_hbm, gain_hbm, route_hbm, weight_hbm, out_ref, *scratch):
    x_ref, gain_ref, route_ref, weight_ref, sems = scratch
    fetch(
        ((x_hbm, x_ref), (gain_hbm, gain_ref), (route_hbm, route_ref), (weight_hbm, weight_ref)),
        sems,
    )
    tokens, width = x_ref.shape
    top = route_ref.shape[0]
    values = x_ref[...].astype(F32)
    center = jnp.mean(values, axis=-1, keepdims=True)
    shifted = values - center
    spread = jnp.mean(jnp.square(shifted), axis=-1, keepdims=True)
    normed = shifted * lax.rsqrt(spread + NORM_EPS) * gain_ref[...]
    out_ref[:, :width] = normed.astype(BF16)
    line = iota((LANES, 1), 0)
    names = route_ref[...].astype(F32)
    high = weight_ref[...].astype(BF16).astype(F32)
    low = weight_ref[...] - high
    extra = jnp.zeros((LANES, tokens), F32)
    for i, part in enumerate((names, high, low)):
        for k in range(top):
            extra = jnp.where(line == i * top + k, part[k : k + 1, :], extra)
    out_ref[:, width:] = jnp.transpose(extra).astype(BF16)


def make_payload(x, gain, routes, weights):
    tokens, width = x.shape
    operands = [
        pltpu.with_memory_space_constraint(o, pltpu.HBM)
        for o in (x, gain.reshape(1, width), routes.T, weights.T)
    ]
    return pl.pallas_call(
        norm_kernel,
        out_shape=jax.ShapeDtypeStruct((tokens, width + LANES), BF16),
        in_specs=[HBM] * 4,
        out_specs=VMEM,
        scratch_shapes=[pltpu.VMEM(o.shape, o.dtype) for o in operands]
        + [pltpu.SemaphoreType.DMA((4,))],
        compiler_params=params(6),
        cost_estimate=cost(1e9),
        name="norm",
    )(*operands)


def slot_match(extra, where_ref, plan, weighted):
    tokens = extra.shape[0]
    top, cap, plane, xor = plan
    lane = iota((1, LANES), 1)
    piece = (2 * lane) ^ where_ref[1] if xor else lane
    target = jnp.where(lane < plane, where_ref[0] + piece, -1).astype(F32)
    named = jnp.zeros((tokens, LANES), F32)
    high = jnp.zeros((tokens, LANES), F32)
    low = jnp.zeros((tokens, LANES), F32)
    for k in range(top):
        hit = extra[:, k : k + 1] == target
        named = jnp.where(hit, 1.0, named)
        if weighted:
            high = jnp.where(hit, extra[:, top + k : top + k + 1], high)
            low = jnp.where(hit, extra[:, 2 * top + k : 2 * top + k + 1], low)
    earlier = (iota((tokens, tokens), 1) < iota((tokens, tokens), 0)).astype(F32).astype(BF16)
    slot = jnp.dot(earlier, named.astype(BF16), preferred_element_type=F32)
    slot = jnp.where(named > 0.5, slot, -1.0)
    columns = plane * cap
    spread = (iota((LANES, columns), 1) // cap == iota((LANES, columns), 0)).astype(F32).astype(BF16)
    place = (iota((1, columns), 1) % cap).astype(F32)
    slot = jnp.dot(slot.astype(BF16), spread, preferred_element_type=F32)
    match = slot == place
    if not weighted:
        return jnp.where(match, 1.0, 0.0)
    high = jnp.dot(high.astype(BF16), spread, preferred_element_type=F32)
    low = jnp.dot(low.astype(BF16), spread, preferred_element_type=F32)
    zero = jnp.zeros_like(high)
    return jnp.where(match, high, zero).astype(BF16), jnp.where(match, low, zero).astype(BF16)


def dispatch_kernel(plan, pieces, count, where_ref, *refs):
    payload_refs, out_refs = refs[:count], refs[-pieces:]
    width = payload_refs[0].shape[1] - LANES
    step = math.gcd(width, 512)
    for j, payload_ref in enumerate(payload_refs):
        extra = payload_ref[:, width:].astype(F32)
        match = slot_match(extra, where_ref, plan, False)
        turned = jnp.transpose(match).astype(BF16)
        rows = turned.shape[0] // pieces
        for left in range(0, width, step):
            block = jnp.dot(turned, payload_ref[:, left : left + step], preferred_element_type=F32)
            block = block.astype(BF16)
            for i in range(pieces):
                out_refs[i][j * rows : (j + 1) * rows, left : left + step] = block[
                    i * rows : (i + 1) * rows
                ]


def dispatch(plan, pieces, where, payloads, after):
    width = payloads[0].shape[1] - LANES
    rows = plan[1] * plan[2] // pieces * len(payloads)
    return pl.pallas_call(
        functools.partial(dispatch_kernel, plan, pieces, len(payloads)),
        out_shape=[jax.ShapeDtypeStruct((rows, width), BF16)] * pieces,
        in_specs=[SMEM] + [VMEM] * len(payloads) + [ANY] * len(after),
        out_specs=[VMEM] * pieces,
        compiler_params=params(8),
        cost_estimate=cost(2e9),
        name="dispatch",
    )(where, *payloads, *after)


def combine_kernel(plan, pieces, count, where_ref, *refs):
    payload_refs, back_refs = refs[:count], refs[count : count + pieces]
    out_refs = refs[-count:]
    width = out_refs[0].shape[1]
    step = math.gcd(width, 512)
    rows = plan[1] * plan[2] // pieces
    for j, payload_ref in enumerate(payload_refs):
        high, low = slot_match(payload_ref[:, width:].astype(F32), where_ref, plan, True)
        spot = slice(j * rows, (j + 1) * rows)
        for left in range(0, width, step):
            cut = slice(left, left + step)
            back = jnp.concatenate([r[spot, cut] for r in back_refs], axis=0)
            total = jnp.dot(high, back, preferred_element_type=F32)
            total = total + jnp.dot(low, back, preferred_element_type=F32)
            out_refs[j][:, cut] = total.astype(out_refs[j].dtype)


def combine(plan, where, payloads, back, after):
    tokens, wide = payloads[0].shape
    width = wide - LANES
    count = len(payloads)
    return pl.pallas_call(
        functools.partial(combine_kernel, plan, len(back), count),
        out_shape=[jax.ShapeDtypeStruct((tokens, width), d) for d in (F32, BF16)[:count]],
        in_specs=[SMEM] + [VMEM] * (count + len(back)) + [ANY] * len(after),
        out_specs=[VMEM] * count,
        compiler_params=params(10),
        cost_estimate=cost(2e9),
        name="combine",
    )(where, *payloads, *back, *after)


def expert_kernel(pieces, gate_ref, up_ref, down_ref, *refs):
    in_refs, out_refs = refs[:pieces], refs[-pieces - 2 : -2]
    x_ref, act_ref = refs[-2:]
    rows = in_refs[0].shape[0]
    hidden = gate_ref.shape[2]
    width = down_ref.shape[2]
    for i in range(pieces):
        x_ref[i * rows : (i + 1) * rows, :] = in_refs[i][...]
    tile = math.gcd(hidden, 256)
    for left in range(0, hidden, tile):
        cut = slice(left, left + tile)
        gate = jnp.dot(x_ref[...], gate_ref[0, :, cut], preferred_element_type=F32)
        lift = jnp.dot(x_ref[...], up_ref[0, :, cut], preferred_element_type=F32)
        gate = jnp.minimum(gate, CLAMP_LIMIT)
        lift = jnp.clip(lift, -CLAMP_LIMIT, CLAMP_LIMIT)
        act = (lift + 1.0) * gate * jax.nn.sigmoid(GATE_SLOPE * gate)
        act_ref[:, cut] = act.astype(BF16)
    wide = math.gcd(width, 512)
    for left in range(0, width, wide):
        cut = slice(left, left + wide)
        done = jnp.dot(act_ref[...], down_ref[0, :, cut], preferred_element_type=F32).astype(BF16)
        for i in range(pieces):
            out_refs[i][:, cut] = done[i * rows : (i + 1) * rows]


def experts(parts, weights, after):
    pieces = len(parts)
    rows, width = parts[0].shape
    hidden = weights[0].shape[2]
    return pl.pallas_call(
        functools.partial(expert_kernel, pieces),
        in_specs=[VMEM] * (3 + pieces) + [ANY] * len(after),
        out_specs=[VMEM] * pieces,
        out_shape=[jax.ShapeDtypeStruct((rows, width), BF16)] * pieces,
        scratch_shapes=[
            pltpu.VMEM((pieces * rows, width), BF16),
            pltpu.VMEM((pieces * rows, hidden), BF16),
        ],
        cost_estimate=pl.CostEstimate(
            flops=6 * pieces * rows * width * hidden,
            transcendentals=0,
            bytes_accessed=4 * pieces * rows * width,
        ),
        compiler_params=params(16),
        name="experts",
    )(*weights, *parts, *after)


def rope_block(x, cos, sin):
    lane = iota((1, LANES), 1)
    quarter = HEAD_DIM // 4
    ahead = pltpu.roll(x, LANES - quarter, axis=1)
    behind = pltpu.roll(x, quarter, axis=1)
    mate = jnp.where(lane % (2 * quarter) < quarter, ahead, behind)
    return x * cos + mate * sin


def attention_kernel(
    first, count, info_ref, sink_ref, table_ref, q_hbm, k_hbm, v_hbm, left_ref, right_ref, after_ref, out_ref,
    k_all, v_all, band_ref, score_ref, chance_ref, q_ref, k_ref, sems,
):
    q_block = WINDOW
    rows = k_hbm.shape[0]
    blocks = rows // q_block
    low, high = max(first, 1), min(first + count + 2, blocks + 1)
    near = slice((low - 1) * q_block, (high - 1) * q_block)
    inside = slice((low - first) * q_block, (high - first) * q_block)
    fetch(
        (
            (k_hbm.at[near, :], k_ref.at[inside, :]),
            (v_hbm.at[near, :], v_all.at[inside, :]),
            (q_hbm.at[first * q_block : (first + count) * q_block, :], q_ref),
        ),
        sems,
    )
    kv_width = k_ref.shape[1]
    pairs = kv_width // LANES
    group = q_ref.shape[1] // kv_width
    span = q_block + 2 * WINDOW
    grid_rows = (rows + 2 * WINDOW) // GRID_W
    per_block = q_block // GRID_W
    lane = iota((1, LANES), 1)
    by_row = lane % HEAD_DIM < HEAD_DIM // 2
    half = lane < HEAD_DIM
    cols = grid_rows
    total = grid_rows + GRID_W
    col_cos = table_ref[cols : cols + GRID_W, :]
    col_sin = table_ref[total + cols : total + cols + GRID_W, :]

    def tables(first, count):
        cos, sin = [], []
        for i in range(count // GRID_W):
            r = first + i
            cos.append(jnp.where(by_row, table_ref[pl.ds(r, 1), :], col_cos))
            sin.append(jnp.where(by_row, table_ref[pl.ds(total + r, 1), :], col_sin))
        return jnp.concatenate(cos, axis=0), jnp.concatenate(sin, axis=0)

    def turn_keys(source, source_row, target_row, count, grid_row):
        cos, sin = tables(grid_row, count)
        for p in range(pairs):
            part = source[pl.ds(source_row, count), p * LANES : (p + 1) * LANES].astype(F32)
            k_all[pl.ds(target_row, count), p * LANES : (p + 1) * LANES] = rope_block(
                part, cos, sin
            ).astype(BF16)

    if first == 0:
        turn_keys(left_ref, 0, 0, q_block, 0)
        v_all[0:q_block, :] = left_ref[:, kv_width:]
    if first + count == blocks:
        slot = (count + 1) * q_block
        turn_keys(right_ref, 0, slot, q_block, (blocks + 1) * per_block)
        v_all[slot : slot + q_block, :] = right_ref[:, kv_width:]

    def keys_step(w, carry):
        at = pl.multiple_of((w - first) * q_block, q_block)
        turn_keys(k_ref, at, at, q_block, w * per_block)
        return carry

    lax.fori_loop(low, high, keys_step, 0)
    gap = iota((q_block, span), 1) - iota((q_block, span), 0)
    band_ref[...] = jnp.where((gap >= 0) & (gap <= 2 * WINDOW), 0.0, MASKED)

    def block_step(b, carry):
        at = pl.multiple_of(b * q_block, q_block)
        block = b + first
        cos, sin = tables((block + 1) * per_block, q_block)
        place = info_ref[0] + block * q_block - WINDOW + iota((1, span), 1)
        bias = band_ref[...] + jnp.where((place >= 0) & (place < info_ref[1]), 0.0, MASKED)
        for p in range(pairs):
            heads = []
            for c in range(group):
                left = (p * group + c) * LANES
                x = q_ref[pl.ds(at, q_block), left : left + LANES].astype(F32)
                x = rope_block(x, cos, sin).astype(BF16).astype(F32) * HEAD_DIM**-0.5
                swapped = pltpu.roll(x, HEAD_DIM, axis=1)
                low_side = c < group // 2
                for one in (x, swapped) if low_side else (swapped, x):
                    keep = half if low_side else jnp.logical_not(half)
                    heads.append(jnp.where(keep, one, 0.0).astype(BF16))
            keys = k_all[pl.ds(at, span), p * LANES : (p + 1) * LANES]
            values = v_all[pl.ds(at, span), p * LANES : (p + 1) * LANES]
            score_ref[p] = lax.dot_general(
                jnp.concatenate(heads, axis=0), keys, (((1,), (1,)), ((), ())),
                preferred_element_type=F32,
            )
            for h in range(2 * group):
                scores = score_ref[p, h * q_block : (h + 1) * q_block, :] + bias
                sink = sink_ref[p * 2 * group + h]
                peak = jnp.maximum(jnp.max(scores, axis=-1, keepdims=True), sink)
                exps = jnp.exp(scores - peak)
                bottom = jnp.sum(exps, axis=-1, keepdims=True) + jnp.exp(sink - peak)
                chance_ref[p, h * q_block : (h + 1) * q_block, :] = (exps * (1.0 / bottom)).astype(
                    BF16
                )
            blended = jnp.dot(chance_ref[p], values, preferred_element_type=F32)
            done = [blended[h * q_block : (h + 1) * q_block] for h in range(2 * group)]
            for c in range(group):
                one, two = done[2 * c], done[2 * c + 1]
                if c < group // 2:
                    two = pltpu.roll(two, HEAD_DIM, axis=1)
                else:
                    one = pltpu.roll(one, HEAD_DIM, axis=1)
                left = (p * group + c) * LANES
                out_ref[pl.ds(at, q_block), left : left + LANES] = jnp.where(
                    half, one, two
                ).astype(BF16)
        return carry

    lax.fori_loop(0, count, block_step, 0)


def rope_table(rows, first_global):
    grid_rows = (rows + 2 * WINDOW) // GRID_W
    quarter = HEAD_DIM // 4
    freqs = ROPE_BASE ** (-jnp.arange(0, HEAD_DIM // 2, 2, dtype=F32) / (HEAD_DIM // 2))
    lane_freq = jnp.tile(freqs, LANES // quarter)
    row_at = (first_global - WINDOW) // GRID_W + jnp.arange(grid_rows, dtype=jnp.int32)
    spots = jnp.concatenate([row_at, jnp.arange(GRID_W, dtype=jnp.int32)]).astype(F32)
    angles = spots[:, None] * lane_freq[None, :]
    sign = jnp.where(jnp.arange(LANES) % (2 * quarter) < quarter, -1.0, 1.0)
    return jnp.concatenate([jnp.cos(angles), jnp.sin(angles) * sign[None, :]], axis=0)


def attention(q, k, v, left, right, sink, table, info, first, count, after):
    rows = q.shape[0]
    kv_width = k.shape[1]
    group = q.shape[1] // kv_width
    assert kv_width % LANES == 0 and group == 2 and rows % WINDOW == 0
    assert rows % GRID_W == 0 and WINDOW % GRID_W == 0
    q_block = WINDOW
    span = q_block + 2 * WINDOW
    heads = q.shape[1] // HEAD_DIM
    done = count * q_block
    return pl.pallas_call(
        functools.partial(attention_kernel, first, count),
        out_shape=jax.ShapeDtypeStruct((done, q.shape[1]), BF16),
        in_specs=[SMEM, SMEM, VMEM] + [HBM] * 3 + [VMEM] * 2 + [ANY],
        out_specs=VMEM,
        scratch_shapes=[
            pltpu.VMEM((done + 2 * WINDOW, kv_width), BF16),
            pltpu.VMEM((done + 2 * WINDOW, kv_width), BF16),
            pltpu.VMEM((q_block, span), F32),
            pltpu.VMEM((kv_width // LANES, 2 * group * q_block, span), F32),
            pltpu.VMEM((kv_width // LANES, 2 * group * q_block, span), BF16),
            pltpu.VMEM((done, q.shape[1]), BF16),
            pltpu.VMEM((done + 2 * WINDOW, kv_width), BF16),
            pltpu.SemaphoreType.DMA((3,)),
        ],
        cost_estimate=pl.CostEstimate(
            flops=24 * done * span * heads * HEAD_DIM,
            transcendentals=done * span * heads,
            bytes_accessed=8 * rows * kv_width * 2,
        ),
        compiler_params=params(16),
        name="attention",
    )(info, sink, table, q, k, v, left, right, after)


def mixer_kernel(rows_ref, weight_hbm, out_ref, weight_ref, total_ref, sems):
    parts, _, part = rows_ref.shape
    width = out_ref.shape[1]
    step = math.gcd(width, 512)
    spots = [slice(i * part, (i + 1) * part) for i in range(parts)]
    loads = [
        pltpu.make_async_copy(weight_hbm.at[spot, :], weight_ref.at[spot, :], sems.at[i])
        for i, spot in enumerate(spots)
    ]
    for load in loads:
        load.start()
    for i, spot in enumerate(spots):
        loads[i].wait()
        for left in range(0, width, step):
            cut = slice(left, left + step)
            total = jnp.dot(rows_ref[i], weight_ref[spot, cut], preferred_element_type=F32)
            if i:
                total = total + total_ref[:, cut]
            if i < parts - 1:
                total_ref[:, cut] = total
            else:
                out_ref[:, cut] = total.astype(BF16)


def mix(rows, weight):
    parts, tokens, _ = rows.shape
    width = weight.shape[1]
    return pl.pallas_call(
        mixer_kernel,
        out_shape=jax.ShapeDtypeStruct((tokens, width), BF16),
        in_specs=[VMEM, HBM],
        out_specs=VMEM,
        scratch_shapes=[
            pltpu.VMEM(weight.shape, BF16),
            pltpu.VMEM((tokens, width), F32),
            pltpu.SemaphoreType.DMA((parts,)),
        ],
        compiler_params=params(18),
        cost_estimate=cost(3e9),
        name="mixer",
    )(rows, pltpu.with_memory_space_constraint(weight, pltpu.HBM))


def relay(x, axis):
    return lax.ppermute(x, axis, [(0, 1), (1, 0)])


def layer(
    queries,
    key_heads,
    value_heads,
    sink_logits,
    mix_weight,
    expert_input,
    norm_gain,
    routes,
    route_weights,
    gate_weight,
    up_weight,
    down_weight,
):
    ring = ("zh", "zl", "xx")
    inner = ("xx", "tp")
    ring_size = lax.axis_size(ring)
    tp_size = lax.axis_size("tp")
    plane = lax.axis_size(inner)
    experts_all = ring_size * tp_size
    tok_local, top = routes.shape
    cap = 2 * tok_local * top // experts_all
    xor = plane <= 8 and plane & (plane - 1) == 0 and plane > 1
    pieces = plane // 2 if xor else 1
    plan = (top, cap, pieces if xor else plane, xor)
    position = lax.axis_index(inner)
    base = lax.axis_index(("zh", "zl")) * plane
    where = jnp.stack([base, position]).astype(jnp.int32)

    def mate(x, step):
        return lax.ppermute(x, inner, [(i, i ^ step) for i in range(plane)])

    def both(x):
        return [x, mate(x, 1)] if xor else [x]

    def exchange(parts):
        if not xor:
            block = parts[0].reshape(-1, plane, cap, parts[0].shape[1]).swapaxes(0, 1)
            turned = lax.all_to_all(block, inner, 0, 0, tiled=True)
            return [turned.swapaxes(0, 1).reshape(parts[0].shape)]
        return [parts[0]] + [mate(parts[p], 2 * p) for p in range(1, pieces)]

    own = make_payload(expert_input, norm_gain, routes, route_weights)
    near = relay(own, "zl")
    far = relay(own, "zh")
    far_near = relay(far, "zl")

    rows_here = queries.shape[0]
    first_global = lax.axis_index(ring) * rows_here
    tail = jnp.concatenate([key_heads[-WINDOW:], value_heads[-WINDOW:]], axis=1)
    head = jnp.concatenate([key_heads[:WINDOW], value_heads[:WINDOW]], axis=1)
    ends = ring_size - 1
    left = lax.ppermute(tail, ring, [(i, i + 1) for i in range(ends)])
    right = lax.ppermute(head, ring, [(i + 1, i) for i in range(ends)])
    table = rope_table(rows_here, first_global)
    info = jnp.stack([first_global, jnp.int32(rows_here * ring_size)]).astype(jnp.int32)
    blocks = rows_here // WINDOW

    def attend(i, after):
        return attention(
            queries, key_heads, value_heads, right if i else left, left if not i else right,
            sink_logits, table, info,
            i * (blocks // 2), blocks // 2, after,
        )

    chunks = [both(x) for x in (own, near, far, far_near)]

    def send(i, after):
        parts = dispatch(plan, pieces, where, chunks[i], after)
        return exchange(parts), parts[0]

    held = [
        pltpu.with_memory_space_constraint(w, pltpu.VMEM)
        for w in (gate_weight, up_weight, down_weight)
    ]

    def work(i, after):
        return experts(arrived[i], held, after)

    arrived, made = {}, {}
    arrived[0], sent = send(0, [])
    arrived[1], sent = send(1, [sent])
    arrived[2], sent = send(2, [sent])
    made[0] = work(0, [sent])
    arrived[3], sent = send(3, [made[0][0]])
    made[1] = work(1, [sent])
    made[2] = work(2, [made[1][0]])
    upper = attend(0, made[2][0])
    made[3] = work(3, [upper])
    lower = attend(1, made[3][0])
    attended = jnp.concatenate([upper, lower], axis=0)

    back = {i: exchange(made[i]) for i in (3, 2, 1, 0)}
    tp_blocks = attended.reshape(tp_size, rows_here // tp_size, attended.shape[1])
    token_rows = lax.all_to_all(tp_blocks, "tp", split_axis=0, concat_axis=0, tiled=True)
    mixer_out = mix(token_rows, mix_weight)

    def gather(i, after):
        own_part, *other = combine(plan, where, chunks[i], back[i], after)
        return [own_part] + [mate(x, 1) for x in other], own_part

    def total(parts):
        return sum(x.astype(F32) for x in parts).astype(BF16)

    parts, done = gather(3, [])
    last = total(parts)
    parts, done = gather(2, [last])
    mid = total(parts + [relay(last, "zl")])
    parts, done = gather(1, [done])
    side = total(parts)
    parts, _ = gather(0, [done])
    summed = total(parts + [relay(side, "zl"), relay(mid, "zh")])
    return (mixer_out, summed)


def solution(mesh):
    n_ep, n_tp = mesh.shape["ep"], mesh.shape["tp"]
    assert n_ep % 4 == 0
    fine = Mesh(mesh.devices.reshape(2, 2, n_ep // 4, n_tp), ("zh", "zl", "xx", "tp"))
    ring = ("zh", "zl", "xx")
    every = ring + ("tp",)
    return jax.shard_map(
        layer,
        mesh=fine,
        in_specs=(
            P(ring, "tp"),
            P(ring, "tp"),
            P(ring, "tp"),
            P("tp"),
            P(),
            P(every, None),
            P(),
            P(every, None),
            P(every, None),
            P(every, None, None),
            P(every, None, None),
            P(every, None, None),
        ),
        out_specs=(P(every, None), P(every, None)),
        check_vma=False,
    )
```

```python
import functools
import math

import jax
import jax.numpy as jnp
from jax import lax
from jax.experimental import pallas as pl
from jax.experimental.pallas import tpu as pltpu
from jax.sharding import Mesh
from jax.sharding import PartitionSpec as P


HEAD_DIM = 64
WINDOW = 128
GRID_W = 64
ROPE_BASE = 10000.0
CLAMP_LIMIT = 7.0
GATE_SLOPE = 1.702
NORM_EPS = 1e-05
LANES = 128
MASKED = -1e30
STRIDE = (2, 1, 2, 1)

VMEM = pl.BlockSpec(memory_space=pltpu.VMEM)
SMEM = pl.BlockSpec(memory_space=pltpu.SMEM)
ANY = pl.BlockSpec(memory_space=pl.ANY)
HBM = pl.BlockSpec(memory_space=pltpu.HBM)
BF16 = jnp.bfloat16
F32 = jnp.float32


def cost(flops):
    return pl.CostEstimate(flops=int(flops), transcendentals=0, bytes_accessed=1 << 20)


def params(mebibytes):
    return pltpu.CompilerParams(vmem_limit_bytes=mebibytes << 20)


def iota(shape, dim):
    return lax.broadcasted_iota(jnp.int32, shape, dim)


def fetch(pairs, sems):
    copies = [pltpu.make_async_copy(s, t, sems.at[i]) for i, (s, t) in enumerate(pairs)]
    for copy in copies:
        copy.start()
    for copy in copies:
        copy.wait()


def norm_kernel(x_hbm, gain_hbm, route_hbm, weight_hbm, out_ref, *scratch):
    x_ref, gain_ref, route_ref, weight_ref, sems = scratch
    fetch(
        ((x_hbm, x_ref), (gain_hbm, gain_ref), (route_hbm, route_ref), (weight_hbm, weight_ref)),
        sems,
    )
    tokens, width = x_ref.shape
    top = route_ref.shape[0]
    values = x_ref[...].astype(F32)
    center = jnp.mean(values, axis=-1, keepdims=True)
    shifted = values - center
    spread = jnp.mean(jnp.square(shifted), axis=-1, keepdims=True)
    normed = shifted * lax.rsqrt(spread + NORM_EPS) * gain_ref[...]
    out_ref[:, :width] = normed.astype(BF16)
    line = iota((LANES, 1), 0)
    names = route_ref[...].astype(F32)
    high = weight_ref[...].astype(BF16).astype(F32)
    low = weight_ref[...] - high
    extra = jnp.zeros((LANES, tokens), F32)
    for i, part in enumerate((names, high, low)):
        for k in range(top):
            extra = jnp.where(line == i * top + k, part[k : k + 1, :], extra)
    out_ref[:, width:] = jnp.transpose(extra).astype(BF16)


def make_payload(x, gain, routes, weights):
    tokens, width = x.shape
    operands = [
        pltpu.with_memory_space_constraint(o, pltpu.HBM)
        for o in (x, gain.reshape(1, width), routes.T, weights.T)
    ]
    return pl.pallas_call(
        norm_kernel,
        out_shape=jax.ShapeDtypeStruct((tokens, width + LANES), BF16),
        in_specs=[HBM] * 4,
        out_specs=VMEM,
        scratch_shapes=[pltpu.VMEM(o.shape, o.dtype) for o in operands]
        + [pltpu.SemaphoreType.DMA((4,))],
        compiler_params=params(6),
        cost_estimate=cost(2e10),
        name="norm",
    )(*operands)


def slot_match(extra, where_ref, plan, weighted):
    tokens = extra.shape[0]
    top, cap, plane, stride = plan
    lane = iota((1, LANES), 1)
    piece = (stride * lane) ^ where_ref[1] if stride else lane
    target = jnp.where(lane < plane, where_ref[0] + piece, -1).astype(F32)
    named = jnp.zeros((tokens, LANES), F32)
    high = jnp.zeros((tokens, LANES), F32)
    low = jnp.zeros((tokens, LANES), F32)
    for k in range(top):
        hit = extra[:, k : k + 1] == target
        named = jnp.where(hit, 1.0, named)
        if weighted:
            high = jnp.where(hit, extra[:, top + k : top + k + 1], high)
            low = jnp.where(hit, extra[:, 2 * top + k : 2 * top + k + 1], low)
    earlier = (iota((tokens, tokens), 1) < iota((tokens, tokens), 0)).astype(F32).astype(BF16)
    slot = jnp.dot(earlier, named.astype(BF16), preferred_element_type=F32)
    slot = jnp.where(named > 0.5, slot, -1.0)
    columns = plane * cap
    spread = (iota((LANES, columns), 1) // cap == iota((LANES, columns), 0)).astype(F32).astype(BF16)
    place = (iota((1, columns), 1) % cap).astype(F32)
    slot = jnp.dot(slot.astype(BF16), spread, preferred_element_type=F32)
    match = slot == place
    if not weighted:
        return jnp.where(match, 1.0, 0.0)
    high = jnp.dot(high.astype(BF16), spread, preferred_element_type=F32)
    low = jnp.dot(low.astype(BF16), spread, preferred_element_type=F32)
    zero = jnp.zeros_like(high)
    return jnp.where(match, high, zero).astype(BF16), jnp.where(match, low, zero).astype(BF16)


def dispatch_kernel(plan, pieces, count, where_ref, *refs):
    payload_refs, out_refs = refs[:count], refs[-pieces:]
    width = payload_refs[0].shape[1] - LANES
    step = math.gcd(width, 512)
    for j, payload_ref in enumerate(payload_refs):
        extra = payload_ref[:, width:].astype(F32)
        match = slot_match(extra, where_ref, plan, False)
        turned = jnp.transpose(match).astype(BF16)
        rows = turned.shape[0] // pieces
        for left in range(0, width, step):
            block = jnp.dot(turned, payload_ref[:, left : left + step], preferred_element_type=F32)
            block = block.astype(BF16)
            for i in range(pieces):
                out_refs[i][j * rows : (j + 1) * rows, left : left + step] = block[
                    i * rows : (i + 1) * rows
                ]


def dispatch(plan, pieces, where, payloads, after):
    width = payloads[0].shape[1] - LANES
    rows = plan[1] * plan[2] // pieces * len(payloads)
    return pl.pallas_call(
        functools.partial(dispatch_kernel, plan, pieces, len(payloads)),
        out_shape=[jax.ShapeDtypeStruct((rows, width), BF16)] * pieces,
        in_specs=[SMEM] + [VMEM] * len(payloads) + [ANY] * len(after),
        out_specs=[VMEM] * pieces,
        compiler_params=params(8),
        cost_estimate=cost(2e10),
        name="dispatch",
    )(where, *payloads, *after)


def combine_kernel(plan, pieces, count, where_ref, *refs):
    payload_refs, back_refs = refs[:count], refs[count : count + pieces]
    out_refs = refs[-count:]
    width = out_refs[0].shape[1]
    step = math.gcd(width, 512)
    rows = plan[1] * plan[2] // pieces
    for j, payload_ref in enumerate(payload_refs):
        high, low = slot_match(payload_ref[:, width:].astype(F32), where_ref, plan, True)
        spot = slice(j * rows, (j + 1) * rows)
        for left in range(0, width, step):
            cut = slice(left, left + step)
            back = jnp.concatenate([r[spot, cut] for r in back_refs], axis=0)
            total = jnp.dot(high, back, preferred_element_type=F32)
            total = total + jnp.dot(low, back, preferred_element_type=F32)
            out_refs[j][:, cut] = total.astype(out_refs[j].dtype)


def combine(plan, where, payloads, back, after):
    tokens, wide = payloads[0].shape
    width = wide - LANES
    count = len(payloads)
    return pl.pallas_call(
        functools.partial(combine_kernel, plan, len(back), count),
        out_shape=[
            jax.ShapeDtypeStruct((tokens, width), d)
            for d in ((F32, BF16) if count > 1 else (BF16,))
        ],
        in_specs=[SMEM] + [VMEM] * (count + len(back)) + [ANY] * len(after),
        out_specs=[VMEM] * count,
        compiler_params=params(10),
        cost_estimate=cost(2e10),
        name="combine",
    )(where, *payloads, *back, *after)


def add_kernel(*refs):
    total = refs[0][...].astype(F32)
    for r in refs[1:-1]:
        total = total + r[...].astype(F32)
    refs[-1][...] = total.astype(BF16)


def add(parts):
    return pl.pallas_call(
        add_kernel,
        out_shape=jax.ShapeDtypeStruct(parts[0].shape, BF16),
        in_specs=[VMEM] * len(parts),
        out_specs=VMEM,
        compiler_params=params(6),
        cost_estimate=cost(2e10),
        name="add",
    )(*parts)


def expert_kernel(pieces, gate_ref, up_ref, down_ref, *refs):
    in_refs, out_refs = refs[:pieces], refs[-pieces - 2 : -2]
    x_ref, act_ref = refs[-2:]
    rows = in_refs[0].shape[0]
    hidden = gate_ref.shape[2]
    width = down_ref.shape[2]
    for i in range(pieces):
        x_ref[i * rows : (i + 1) * rows, :] = in_refs[i][...]
    tile = math.gcd(hidden, 256)
    for left in range(0, hidden, tile):
        cut = slice(left, left + tile)
        gate = jnp.dot(x_ref[...], gate_ref[0, :, cut], preferred_element_type=F32)
        lift = jnp.dot(x_ref[...], up_ref[0, :, cut], preferred_element_type=F32)
        gate = jnp.minimum(gate, CLAMP_LIMIT)
        lift = jnp.clip(lift, -CLAMP_LIMIT, CLAMP_LIMIT)
        act = (lift + 1.0) * gate * jax.nn.sigmoid(GATE_SLOPE * gate)
        act_ref[:, cut] = act.astype(BF16)
    wide = math.gcd(width, 512)
    for left in range(0, width, wide):
        cut = slice(left, left + wide)
        done = jnp.dot(act_ref[...], down_ref[0, :, cut], preferred_element_type=F32).astype(BF16)
        for i in range(pieces):
            out_refs[i][:, cut] = done[i * rows : (i + 1) * rows]


def experts(parts, weights, after):
    pieces = len(parts)
    rows, width = parts[0].shape
    hidden = weights[0].shape[2]
    return pl.pallas_call(
        functools.partial(expert_kernel, pieces),
        in_specs=[VMEM] * (3 + pieces) + [ANY] * len(after),
        out_specs=[VMEM] * pieces,
        out_shape=[jax.ShapeDtypeStruct((rows, width), BF16)] * pieces,
        scratch_shapes=[
            pltpu.VMEM((pieces * rows, width), BF16),
            pltpu.VMEM((pieces * rows, hidden), BF16),
        ],
        cost_estimate=pl.CostEstimate(
            flops=6 * pieces * rows * width * hidden,
            transcendentals=0,
            bytes_accessed=4 * pieces * rows * width,
        ),
        compiler_params=params(16),
        name="experts",
    )(*weights, *parts, *after)


def rope_block(x, cos, sin):
    lane = iota((1, LANES), 1)
    quarter = HEAD_DIM // 4
    ahead = pltpu.roll(x, LANES - quarter, axis=1)
    behind = pltpu.roll(x, quarter, axis=1)
    mate = jnp.where(lane % (2 * quarter) < quarter, ahead, behind)
    return x * cos + mate * sin


def attention_kernel(
    first, count, info_ref, sink_ref, table_ref, q_hbm, k_hbm, v_hbm, left_ref, right_ref, after_ref, out_ref,
    k_all, v_all, band_ref, score_ref, chance_ref, q_ref, k_ref, sems,
):
    q_block = WINDOW
    rows = k_hbm.shape[0]
    blocks = rows // q_block
    low, high = max(first, 1), min(first + count + 2, blocks + 1)
    near = slice((low - 1) * q_block, (high - 1) * q_block)
    inside = slice((low - first) * q_block, (high - first) * q_block)
    fetch(
        (
            (k_hbm.at[near, :], k_ref.at[inside, :]),
            (v_hbm.at[near, :], v_all.at[inside, :]),
            (q_hbm.at[first * q_block : (first + count) * q_block, :], q_ref),
        ),
        sems,
    )
    kv_width = k_ref.shape[1]
    pairs = kv_width // LANES
    group = q_ref.shape[1] // kv_width
    span = q_block + 2 * WINDOW
    grid_rows = (rows + 2 * WINDOW) // GRID_W
    per_block = q_block // GRID_W
    lane = iota((1, LANES), 1)
    by_row = lane % HEAD_DIM < HEAD_DIM // 2
    half = lane < HEAD_DIM
    cols = grid_rows
    total = grid_rows + GRID_W
    col_cos = table_ref[cols : cols + GRID_W, :]
    col_sin = table_ref[total + cols : total + cols + GRID_W, :]

    def tables(first, count):
        cos, sin = [], []
        for i in range(count // GRID_W):
            r = first + i
            cos.append(jnp.where(by_row, table_ref[pl.ds(r, 1), :], col_cos))
            sin.append(jnp.where(by_row, table_ref[pl.ds(total + r, 1), :], col_sin))
        return jnp.concatenate(cos, axis=0), jnp.concatenate(sin, axis=0)

    def turn_keys(source, source_row, target_row, count, grid_row):
        cos, sin = tables(grid_row, count)
        for p in range(pairs):
            part = source[pl.ds(source_row, count), p * LANES : (p + 1) * LANES].astype(F32)
            k_all[pl.ds(target_row, count), p * LANES : (p + 1) * LANES] = rope_block(
                part, cos, sin
            ).astype(BF16)

    if first == 0:
        turn_keys(left_ref, 0, 0, q_block, 0)
        v_all[0:q_block, :] = left_ref[:, kv_width:]
    if first + count == blocks:
        slot = (count + 1) * q_block
        turn_keys(right_ref, 0, slot, q_block, (blocks + 1) * per_block)
        v_all[slot : slot + q_block, :] = right_ref[:, kv_width:]

    def keys_step(w, carry):
        at = pl.multiple_of((w - first) * q_block, q_block)
        turn_keys(k_ref, at, at, q_block, w * per_block)
        return carry

    lax.fori_loop(low, high, keys_step, 0)
    gap = iota((q_block, span), 1) - iota((q_block, span), 0)
    band_ref[...] = jnp.where((gap >= 0) & (gap <= 2 * WINDOW), 0.0, MASKED)

    def block_step(b, carry):
        at = pl.multiple_of(b * q_block, q_block)
        block = b + first
        cos, sin = tables((block + 1) * per_block, q_block)
        place = info_ref[0] + block * q_block - WINDOW + iota((1, span), 1)
        bias = band_ref[...] + jnp.where((place >= 0) & (place < info_ref[1]), 0.0, MASKED)
        for p in range(pairs):
            heads = []
            for c in range(group):
                left = (p * group + c) * LANES
                x = q_ref[pl.ds(at, q_block), left : left + LANES].astype(F32)
                x = rope_block(x, cos, sin).astype(BF16).astype(F32) * HEAD_DIM**-0.5
                swapped = pltpu.roll(x, HEAD_DIM, axis=1)
                low_side = c < group // 2
                for one in (x, swapped) if low_side else (swapped, x):
                    keep = half if low_side else jnp.logical_not(half)
                    heads.append(jnp.where(keep, one, 0.0).astype(BF16))
            keys = k_all[pl.ds(at, span), p * LANES : (p + 1) * LANES]
            values = v_all[pl.ds(at, span), p * LANES : (p + 1) * LANES]
            score_ref[p] = lax.dot_general(
                jnp.concatenate(heads, axis=0), keys, (((1,), (1,)), ((), ())),
                preferred_element_type=F32,
            )
            for h in range(2 * group):
                scores = score_ref[p, h * q_block : (h + 1) * q_block, :] + bias
                sink = sink_ref[p * 2 * group + h]
                peak = jnp.maximum(jnp.max(scores, axis=-1, keepdims=True), sink)
                exps = jnp.exp(scores - peak)
                bottom = jnp.sum(exps, axis=-1, keepdims=True) + jnp.exp(sink - peak)
                chance_ref[p, h * q_block : (h + 1) * q_block, :] = (exps * (1.0 / bottom)).astype(
                    BF16
                )
            blended = jnp.dot(chance_ref[p], values, preferred_element_type=F32)
            done = [blended[h * q_block : (h + 1) * q_block] for h in range(2 * group)]
            for c in range(group):
                one, two = done[2 * c], done[2 * c + 1]
                if c < group // 2:
                    two = pltpu.roll(two, HEAD_DIM, axis=1)
                else:
                    one = pltpu.roll(one, HEAD_DIM, axis=1)
                left = (p * group + c) * LANES
                out_ref[pl.ds(at, q_block), left : left + LANES] = jnp.where(
                    half, one, two
                ).astype(BF16)
        return carry

    lax.fori_loop(0, count, block_step, 0)


def rope_table(rows, first_global):
    grid_rows = (rows + 2 * WINDOW) // GRID_W
    quarter = HEAD_DIM // 4
    freqs = ROPE_BASE ** (-jnp.arange(0, HEAD_DIM // 2, 2, dtype=F32) / (HEAD_DIM // 2))
    lane_freq = jnp.tile(freqs, LANES // quarter)
    row_at = (first_global - WINDOW) // GRID_W + jnp.arange(grid_rows, dtype=jnp.int32)
    spots = jnp.concatenate([row_at, jnp.arange(GRID_W, dtype=jnp.int32)]).astype(F32)
    angles = spots[:, None] * lane_freq[None, :]
    sign = jnp.where(jnp.arange(LANES) % (2 * quarter) < quarter, -1.0, 1.0)
    return jnp.concatenate([jnp.cos(angles), jnp.sin(angles) * sign[None, :]], axis=0)


def attention(q, k, v, left, right, sink, table, info, first, count, after):
    rows = q.shape[0]
    kv_width = k.shape[1]
    group = q.shape[1] // kv_width
    assert kv_width % LANES == 0 and group == 2 and rows % WINDOW == 0
    assert rows % GRID_W == 0 and WINDOW % GRID_W == 0
    q_block = WINDOW
    span = q_block + 2 * WINDOW
    heads = q.shape[1] // HEAD_DIM
    done = count * q_block
    return pl.pallas_call(
        functools.partial(attention_kernel, first, count),
        out_shape=jax.ShapeDtypeStruct((done, q.shape[1]), BF16),
        in_specs=[SMEM, SMEM, VMEM] + [HBM] * 3 + [VMEM] * 2 + [ANY],
        out_specs=VMEM,
        scratch_shapes=[
            pltpu.VMEM((done + 2 * WINDOW, kv_width), BF16),
            pltpu.VMEM((done + 2 * WINDOW, kv_width), BF16),
            pltpu.VMEM((q_block, span), F32),
            pltpu.VMEM((kv_width // LANES, 2 * group * q_block, span), F32),
            pltpu.VMEM((kv_width // LANES, 2 * group * q_block, span), BF16),
            pltpu.VMEM((done, q.shape[1]), BF16),
            pltpu.VMEM((done + 2 * WINDOW, kv_width), BF16),
            pltpu.SemaphoreType.DMA((3,)),
        ],
        cost_estimate=pl.CostEstimate(
            flops=24 * done * span * heads * HEAD_DIM,
            transcendentals=done * span * heads,
            bytes_accessed=8 * rows * kv_width * 2,
        ),
        compiler_params=params(16),
        name="attention",
    )(info, sink, table, q, k, v, left, right, after)


def mixer_kernel(rows_ref, weight_hbm, out_ref, weight_ref, total_ref, sems):
    parts, _, part = rows_ref.shape
    width = out_ref.shape[1]
    step = math.gcd(width, 512)
    spots = [slice(i * part, (i + 1) * part) for i in range(parts)]
    loads = [
        pltpu.make_async_copy(weight_hbm.at[spot, :], weight_ref.at[spot, :], sems.at[i])
        for i, spot in enumerate(spots)
    ]
    for load in loads:
        load.start()
    for i, spot in enumerate(spots):
        loads[i].wait()
        for left in range(0, width, step):
            cut = slice(left, left + step)
            total = jnp.dot(rows_ref[i], weight_ref[spot, cut], preferred_element_type=F32)
            if i:
                total = total + total_ref[:, cut]
            if i < parts - 1:
                total_ref[:, cut] = total
            else:
                out_ref[:, cut] = total.astype(BF16)


def mix(rows, weight):
    parts, tokens, _ = rows.shape
    width = weight.shape[1]
    return pl.pallas_call(
        mixer_kernel,
        out_shape=jax.ShapeDtypeStruct((tokens, width), BF16),
        in_specs=[VMEM, HBM],
        out_specs=VMEM,
        scratch_shapes=[
            pltpu.VMEM(weight.shape, BF16),
            pltpu.VMEM((tokens, width), F32),
            pltpu.SemaphoreType.DMA((parts,)),
        ],
        compiler_params=params(18),
        cost_estimate=cost(2e10),
        name="mixer",
    )(rows, pltpu.with_memory_space_constraint(weight, pltpu.HBM))


def relay(x, axis):
    return lax.ppermute(x, axis, [(0, 1), (1, 0)])


def layer(
    queries,
    key_heads,
    value_heads,
    sink_logits,
    mix_weight,
    expert_input,
    norm_gain,
    routes,
    route_weights,
    gate_weight,
    up_weight,
    down_weight,
):
    ring = ("zh", "zl", "xx")
    inner = ("xx", "tp")
    ring_size = lax.axis_size(ring)
    tp_size = lax.axis_size("tp")
    plane = lax.axis_size(inner)
    experts_all = ring_size * tp_size
    tok_local, top = routes.shape
    cap = 2 * tok_local * top // experts_all
    xor = plane <= 8 and plane & (plane - 1) == 0 and plane > 1

    def layout(i):
        if not xor:
            return 1, (top, cap, plane, 0)
        stride = STRIDE[i]
        return plane // stride, (top, cap, plane // stride, stride)

    position = lax.axis_index(inner)
    base = lax.axis_index(("zh", "zl")) * plane
    where = jnp.stack([base, position]).astype(jnp.int32)

    def mate(x, step):
        return lax.ppermute(x, inner, [(i, i ^ step) for i in range(plane)])

    def both(x, i):
        return [x, mate(x, 1)] if layout(i)[1][3] == 2 else [x]

    def exchange(parts, i):
        if not xor:
            block = parts[0].reshape(-1, plane, cap, parts[0].shape[1]).swapaxes(0, 1)
            turned = lax.all_to_all(block, inner, 0, 0, tiled=True)
            return [turned.swapaxes(0, 1).reshape(parts[0].shape)]
        stride = layout(i)[1][3]
        return [parts[0]] + [mate(parts[p], stride * p) for p in range(1, len(parts))]

    own = make_payload(expert_input, norm_gain, routes, route_weights)
    near = relay(own, "zl")
    far = relay(own, "zh")
    far_near = relay(far, "zl")

    rows_here = queries.shape[0]
    first_global = lax.axis_index(ring) * rows_here
    tail = jnp.concatenate([key_heads[-WINDOW:], value_heads[-WINDOW:]], axis=1)
    head = jnp.concatenate([key_heads[:WINDOW], value_heads[:WINDOW]], axis=1)
    ends = ring_size - 1
    left = lax.ppermute(tail, ring, [(i, i + 1) for i in range(ends)])
    right = lax.ppermute(head, ring, [(i + 1, i) for i in range(ends)])
    table = rope_table(rows_here, first_global)
    info = jnp.stack([first_global, jnp.int32(rows_here * ring_size)]).astype(jnp.int32)
    blocks = rows_here // WINDOW

    half = (blocks - 2) // 2
    ranges = ((1, half), (1 + half, blocks - 2 - half), (0, 1), (blocks - 1, 1))

    def attend(i, after):
        first, count = ranges[i]
        return attention(
            queries, key_heads, value_heads, left if i == 2 else table,
            right if i == 3 else table, sink_logits, table, info, first, count, after,
        )

    chunks = [both(x, i) for i, x in enumerate((own, near, far, far_near))]

    def send(i, after):
        pieces, plan = layout(i)
        parts = dispatch(plan, pieces, where, chunks[i], after)
        return exchange(parts, i), parts[0]

    held = [
        pltpu.with_memory_space_constraint(w, pltpu.VMEM)
        for w in (gate_weight, up_weight, down_weight)
    ]

    def work(i, after):
        return experts(arrived[i], held, after)

    arrived, made, rows = {}, {}, {}
    arrived[0], sent = send(0, [table, info])
    rows[0] = attend(0, sent)
    arrived[1], sent = send(1, [rows[0]])
    made[0] = work(0, [sent])
    arrived[2], sent = send(2, [made[0][0]])
    made[1] = work(1, [sent])
    arrived[3], sent = send(3, [made[1][0]])
    made[2] = work(2, [sent])
    rows[1] = attend(1, made[2][0])
    made[3] = work(3, [rows[1]])
    rows[3] = attend(3, made[3][0])
    rows[2] = attend(2, rows[3])
    attended = jnp.concatenate([rows[i] for i in (2, 0, 1, 3)], axis=0)

    back = {i: exchange(made[i], i) for i in (3, 2, 1, 0)}
    tp_blocks = attended.reshape(tp_size, rows_here // tp_size, attended.shape[1])
    token_rows = lax.all_to_all(tp_blocks, "tp", split_axis=0, concat_axis=0, tiled=True)

    def gather(i, after):
        own_part, *other = combine(layout(i)[1], where, chunks[i], back[i], after)
        return [own_part] + [mate(x, 1) for x in other], own_part

    parts, done = gather(3, [])
    last = add(parts) if len(parts) > 1 else parts[0].astype(BF16)
    parts, done = gather(2, [last])
    mid = add(parts + [relay(last, "zl")])
    parts, done = gather(1, [done])
    side = add(parts) if len(parts) > 1 else parts[0].astype(BF16)
    parts, _ = gather(0, [done])
    mixer_out = mix(token_rows, mix_weight)
    summed = add(parts + [relay(side, "zl"), relay(mid, "zh")])
    return (mixer_out, summed)


def solution(mesh):
    n_ep, n_tp = mesh.shape["ep"], mesh.shape["tp"]
    assert n_ep % 4 == 0
    fine = Mesh(mesh.devices.reshape(2, 2, n_ep // 4, n_tp), ("zh", "zl", "xx", "tp"))
    ring = ("zh", "zl", "xx")
    every = ring + ("tp",)
    return jax.shard_map(
        layer,
        mesh=fine,
        in_specs=(
            P(ring, "tp"),
            P(ring, "tp"),
            P(ring, "tp"),
            P("tp"),
            P(),
            P(every, None),
            P(),
            P(every, None),
            P(every, None),
            P(every, None, None),
            P(every, None, None),
            P(every, None, None),
        ),
        out_specs=(P(every, None), P(every, None)),
        check_vma=False,
    )
```

```python
import functools
import math

import jax
import jax.numpy as jnp
from jax import lax
from jax.experimental import pallas as pl
from jax.experimental.pallas import tpu as pltpu
from jax.sharding import Mesh
from jax.sharding import PartitionSpec as P


HEAD_DIM = 64
WINDOW = 128
GRID_W = 64
ROPE_BASE = 10000.0
CLAMP_LIMIT = 7.0
GATE_SLOPE = 1.702
NORM_EPS = 1e-05
LANES = 128
MASKED = -1e30
STRIDE = (2, 1, 2, 1)

VMEM = pl.BlockSpec(memory_space=pltpu.VMEM)
SMEM = pl.BlockSpec(memory_space=pltpu.SMEM)
ANY = pl.BlockSpec(memory_space=pl.ANY)
HBM = pl.BlockSpec(memory_space=pltpu.HBM)
BF16 = jnp.bfloat16
F32 = jnp.float32


def cost(flops):
    return pl.CostEstimate(flops=int(flops), transcendentals=0, bytes_accessed=1 << 20)


def params(mebibytes):
    return pltpu.CompilerParams(vmem_limit_bytes=mebibytes << 20)


def iota(shape, dim):
    return lax.broadcasted_iota(jnp.int32, shape, dim)


def fetch(pairs, sems):
    copies = [pltpu.make_async_copy(s, t, sems.at[i]) for i, (s, t) in enumerate(pairs)]
    for copy in copies:
        copy.start()
    for copy in copies:
        copy.wait()


def norm_kernel(x_hbm, gain_hbm, route_hbm, weight_hbm, out_ref, *scratch):
    x_ref, gain_ref, route_ref, weight_ref, sems = scratch
    fetch(
        ((x_hbm, x_ref), (gain_hbm, gain_ref), (route_hbm, route_ref), (weight_hbm, weight_ref)),
        sems,
    )
    tokens, width = x_ref.shape
    top = route_ref.shape[0]
    values = x_ref[...].astype(F32)
    center = jnp.mean(values, axis=-1, keepdims=True)
    shifted = values - center
    spread = jnp.mean(jnp.square(shifted), axis=-1, keepdims=True)
    normed = shifted * lax.rsqrt(spread + NORM_EPS) * gain_ref[...]
    out_ref[:, :width] = normed.astype(BF16)
    line = iota((LANES, 1), 0)
    names = route_ref[...].astype(F32)
    high = weight_ref[...].astype(BF16).astype(F32)
    low = weight_ref[...] - high
    extra = jnp.zeros((LANES, tokens), F32)
    for i, part in enumerate((names, high, low)):
        for k in range(top):
            extra = jnp.where(line == i * top + k, part[k : k + 1, :], extra)
    out_ref[:, width:] = jnp.transpose(extra).astype(BF16)


def make_payload(x, gain, routes, weights):
    tokens, width = x.shape
    operands = [
        pltpu.with_memory_space_constraint(o, pltpu.HBM)
        for o in (x, gain.reshape(1, width), routes.T, weights.T)
    ]
    return pl.pallas_call(
        norm_kernel,
        out_shape=jax.ShapeDtypeStruct((tokens, width + LANES), BF16),
        in_specs=[HBM] * 4,
        out_specs=VMEM,
        scratch_shapes=[pltpu.VMEM(o.shape, o.dtype) for o in operands]
        + [pltpu.SemaphoreType.DMA((4,))],
        compiler_params=params(6),
        cost_estimate=cost(2e10),
        name="norm",
    )(*operands)


def slot_match(extra, where_ref, plan, weighted):
    tokens = extra.shape[0]
    top, cap, plane, stride = plan
    lane = iota((1, LANES), 1)
    piece = (stride * lane) ^ where_ref[1] if stride else lane
    target = jnp.where(lane < plane, where_ref[0] + piece, -1).astype(F32)
    named = jnp.zeros((tokens, LANES), F32)
    high = jnp.zeros((tokens, LANES), F32)
    low = jnp.zeros((tokens, LANES), F32)
    for k in range(top):
        hit = extra[:, k : k + 1] == target
        named = jnp.where(hit, 1.0, named)
        if weighted:
            high = jnp.where(hit, extra[:, top + k : top + k + 1], high)
            low = jnp.where(hit, extra[:, 2 * top + k : 2 * top + k + 1], low)
    earlier = (iota((tokens, tokens), 1) < iota((tokens, tokens), 0)).astype(F32).astype(BF16)
    slot = jnp.dot(earlier, named.astype(BF16), preferred_element_type=F32)
    slot = jnp.where(named > 0.5, slot, -1.0)
    columns = plane * cap
    spread = (iota((LANES, columns), 1) // cap == iota((LANES, columns), 0)).astype(F32).astype(BF16)
    place = (iota((1, columns), 1) % cap).astype(F32)
    slot = jnp.dot(slot.astype(BF16), spread, preferred_element_type=F32)
    match = slot == place
    if not weighted:
        return jnp.where(match, 1.0, 0.0)
    high = jnp.dot(high.astype(BF16), spread, preferred_element_type=F32)
    low = jnp.dot(low.astype(BF16), spread, preferred_element_type=F32)
    zero = jnp.zeros_like(high)
    return jnp.where(match, high, zero).astype(BF16), jnp.where(match, low, zero).astype(BF16)


def dispatch_kernel(plan, pieces, count, where_ref, *refs):
    payload_refs, out_refs = refs[:count], refs[-pieces:]
    width = payload_refs[0].shape[1] - LANES
    step = math.gcd(width, 512)
    for j, payload_ref in enumerate(payload_refs):
        extra = payload_ref[:, width:].astype(F32)
        match = slot_match(extra, where_ref, plan, False)
        turned = jnp.transpose(match).astype(BF16)
        rows = turned.shape[0] // pieces
        for left in range(0, width, step):
            block = jnp.dot(turned, payload_ref[:, left : left + step], preferred_element_type=F32)
            block = block.astype(BF16)
            for i in range(pieces):
                out_refs[i][j * rows : (j + 1) * rows, left : left + step] = block[
                    i * rows : (i + 1) * rows
                ]


def dispatch(plan, pieces, where, payloads, after):
    width = payloads[0].shape[1] - LANES
    rows = plan[1] * plan[2] // pieces * len(payloads)
    return pl.pallas_call(
        functools.partial(dispatch_kernel, plan, pieces, len(payloads)),
        out_shape=[jax.ShapeDtypeStruct((rows, width), BF16)] * pieces,
        in_specs=[SMEM] + [VMEM] * len(payloads) + [ANY] * len(after),
        out_specs=[VMEM] * pieces,
        compiler_params=params(8),
        cost_estimate=cost(2e10),
        name="dispatch",
    )(where, *payloads, *after)


def combine_kernel(plan, pieces, count, where_ref, *refs):
    payload_refs, back_refs = refs[:count], refs[count : count + pieces]
    out_refs = refs[-count:]
    width = out_refs[0].shape[1]
    step = math.gcd(width, 512)
    rows = plan[1] * plan[2] // pieces
    for j, payload_ref in enumerate(payload_refs):
        high, low = slot_match(payload_ref[:, width:].astype(F32), where_ref, plan, True)
        spot = slice(j * rows, (j + 1) * rows)
        for left in range(0, width, step):
            cut = slice(left, left + step)
            back = jnp.concatenate([r[spot, cut] for r in back_refs], axis=0)
            total = jnp.dot(high, back, preferred_element_type=F32)
            total = total + jnp.dot(low, back, preferred_element_type=F32)
            out_refs[j][:, cut] = total.astype(out_refs[j].dtype)


def combine(plan, where, payloads, back, after):
    tokens, wide = payloads[0].shape
    width = wide - LANES
    count = len(payloads)
    return pl.pallas_call(
        functools.partial(combine_kernel, plan, len(back), count),
        out_shape=[
            jax.ShapeDtypeStruct((tokens, width), d)
            for d in ((F32, BF16) if count > 1 else (BF16,))
        ],
        in_specs=[SMEM] + [VMEM] * (count + len(back)) + [ANY] * len(after),
        out_specs=[VMEM] * count,
        compiler_params=params(10),
        cost_estimate=cost(2e10),
        name="combine",
    )(where, *payloads, *back, *after)


def add_kernel(*refs):
    total = refs[0][...].astype(F32)
    for r in refs[1:-1]:
        total = total + r[...].astype(F32)
    refs[-1][...] = total.astype(BF16)


def add(parts):
    return pl.pallas_call(
        add_kernel,
        out_shape=jax.ShapeDtypeStruct(parts[0].shape, BF16),
        in_specs=[VMEM] * len(parts),
        out_specs=VMEM,
        compiler_params=params(6),
        cost_estimate=cost(2e10),
        name="add",
    )(*parts)


def expert_kernel(pieces, gate_ref, up_ref, down_ref, *refs):
    in_refs, out_refs = refs[:pieces], refs[-pieces - 2 : -2]
    x_ref, act_ref = refs[-2:]
    rows = in_refs[0].shape[0]
    hidden = gate_ref.shape[2]
    width = down_ref.shape[2]
    for i in range(pieces):
        x_ref[i * rows : (i + 1) * rows, :] = in_refs[i][...]
    tile = math.gcd(hidden, 256)
    for left in range(0, hidden, tile):
        cut = slice(left, left + tile)
        gate = jnp.dot(x_ref[...], gate_ref[0, :, cut], preferred_element_type=F32)
        lift = jnp.dot(x_ref[...], up_ref[0, :, cut], preferred_element_type=F32)
        gate = jnp.minimum(gate, CLAMP_LIMIT)
        lift = jnp.clip(lift, -CLAMP_LIMIT, CLAMP_LIMIT)
        act = (lift + 1.0) * gate * jax.nn.sigmoid(GATE_SLOPE * gate)
        act_ref[:, cut] = act.astype(BF16)
    wide = math.gcd(width, 512)
    for left in range(0, width, wide):
        cut = slice(left, left + wide)
        done = jnp.dot(act_ref[...], down_ref[0, :, cut], preferred_element_type=F32).astype(BF16)
        for i in range(pieces):
            out_refs[i][:, cut] = done[i * rows : (i + 1) * rows]


def experts(parts, weights, after):
    pieces = len(parts)
    rows, width = parts[0].shape
    hidden = weights[0].shape[2]
    return pl.pallas_call(
        functools.partial(expert_kernel, pieces),
        in_specs=[VMEM] * (3 + pieces) + [ANY] * len(after),
        out_specs=[VMEM] * pieces,
        out_shape=[jax.ShapeDtypeStruct((rows, width), BF16)] * pieces,
        scratch_shapes=[
            pltpu.VMEM((pieces * rows, width), BF16),
            pltpu.VMEM((pieces * rows, hidden), BF16),
        ],
        cost_estimate=pl.CostEstimate(
            flops=6 * pieces * rows * width * hidden,
            transcendentals=0,
            bytes_accessed=4 * pieces * rows * width,
        ),
        compiler_params=params(16),
        name="experts",
    )(*weights, *parts, *after)


def rope_block(x, cos, sin):
    lane = iota((1, LANES), 1)
    quarter = HEAD_DIM // 4
    ahead = pltpu.roll(x, LANES - quarter, axis=1)
    behind = pltpu.roll(x, quarter, axis=1)
    mate = jnp.where(lane % (2 * quarter) < quarter, ahead, behind)
    return x * cos + mate * sin


def attention_kernel(
    first, count, info_ref, sink_ref, table_ref, q_hbm, k_hbm, v_hbm, left_ref, right_ref, after_ref, out_ref,
    k_all, v_all, band_ref, score_ref, chance_ref, q_ref, k_ref, sems,
):
    q_block = WINDOW
    rows = k_hbm.shape[0]
    blocks = rows // q_block
    low, high = max(first, 1), min(first + count + 2, blocks + 1)
    near = slice((low - 1) * q_block, (high - 1) * q_block)
    inside = slice((low - first) * q_block, (high - first) * q_block)
    fetch(
        (
            (k_hbm.at[near, :], k_ref.at[inside, :]),
            (v_hbm.at[near, :], v_all.at[inside, :]),
            (q_hbm.at[first * q_block : (first + count) * q_block, :], q_ref),
        ),
        sems,
    )
    kv_width = k_ref.shape[1]
    pairs = kv_width // LANES
    group = q_ref.shape[1] // kv_width
    span = q_block + 2 * WINDOW
    grid_rows = (rows + 2 * WINDOW) // GRID_W
    per_block = q_block // GRID_W
    lane = iota((1, LANES), 1)
    by_row = lane % HEAD_DIM < HEAD_DIM // 2
    half = lane < HEAD_DIM
    cols = grid_rows
    total = grid_rows + GRID_W
    col_cos = table_ref[cols : cols + GRID_W, :]
    col_sin = table_ref[total + cols : total + cols + GRID_W, :]

    def tables(first, count):
        cos, sin = [], []
        for i in range(count // GRID_W):
            r = first + i
            cos.append(jnp.where(by_row, table_ref[pl.ds(r, 1), :], col_cos))
            sin.append(jnp.where(by_row, table_ref[pl.ds(total + r, 1), :], col_sin))
        return jnp.concatenate(cos, axis=0), jnp.concatenate(sin, axis=0)

    def turn_keys(source, source_row, target_row, count, grid_row):
        cos, sin = tables(grid_row, count)
        for p in range(pairs):
            part = source[pl.ds(source_row, count), p * LANES : (p + 1) * LANES].astype(F32)
            k_all[pl.ds(target_row, count), p * LANES : (p + 1) * LANES] = rope_block(
                part, cos, sin
            ).astype(BF16)

    if first == 0:
        turn_keys(left_ref, 0, 0, q_block, 0)
        v_all[0:q_block, :] = left_ref[:, kv_width:]
    if first + count == blocks:
        slot = (count + 1) * q_block
        turn_keys(right_ref, 0, slot, q_block, (blocks + 1) * per_block)
        v_all[slot : slot + q_block, :] = right_ref[:, kv_width:]

    def keys_step(w, carry):
        at = pl.multiple_of((w - first) * q_block, q_block)
        turn_keys(k_ref, at, at, q_block, w * per_block)
        return carry

    lax.fori_loop(low, high, keys_step, 0)
    gap = iota((q_block, span), 1) - iota((q_block, span), 0)
    band_ref[...] = jnp.where((gap >= 0) & (gap <= 2 * WINDOW), 0.0, MASKED)

    def block_step(b, carry):
        at = pl.multiple_of(b * q_block, q_block)
        block = b + first
        cos, sin = tables((block + 1) * per_block, q_block)
        place = info_ref[0] + block * q_block - WINDOW + iota((1, span), 1)
        bias = band_ref[...] + jnp.where((place >= 0) & (place < info_ref[1]), 0.0, MASKED)
        for p in range(pairs):
            heads = []
            for c in range(group):
                left = (p * group + c) * LANES
                x = q_ref[pl.ds(at, q_block), left : left + LANES].astype(F32)
                x = rope_block(x, cos, sin).astype(BF16).astype(F32) * HEAD_DIM**-0.5
                swapped = pltpu.roll(x, HEAD_DIM, axis=1)
                low_side = c < group // 2
                for one in (x, swapped) if low_side else (swapped, x):
                    keep = half if low_side else jnp.logical_not(half)
                    heads.append(jnp.where(keep, one, 0.0).astype(BF16))
            keys = k_all[pl.ds(at, span), p * LANES : (p + 1) * LANES]
            values = v_all[pl.ds(at, span), p * LANES : (p + 1) * LANES]
            score_ref[p] = lax.dot_general(
                jnp.concatenate(heads, axis=0), keys, (((1,), (1,)), ((), ())),
                preferred_element_type=F32,
            )
            for h in range(2 * group):
                scores = score_ref[p, h * q_block : (h + 1) * q_block, :] + bias
                sink = sink_ref[p * 2 * group + h]
                peak = jnp.maximum(jnp.max(scores, axis=-1, keepdims=True), sink)
                exps = jnp.exp(scores - peak)
                bottom = jnp.sum(exps, axis=-1, keepdims=True) + jnp.exp(sink - peak)
                chance_ref[p, h * q_block : (h + 1) * q_block, :] = (exps * (1.0 / bottom)).astype(
                    BF16
                )
            blended = jnp.dot(chance_ref[p], values, preferred_element_type=F32)
            done = [blended[h * q_block : (h + 1) * q_block] for h in range(2 * group)]
            for c in range(group):
                one, two = done[2 * c], done[2 * c + 1]
                if c < group // 2:
                    two = pltpu.roll(two, HEAD_DIM, axis=1)
                else:
                    one = pltpu.roll(one, HEAD_DIM, axis=1)
                left = (p * group + c) * LANES
                out_ref[pl.ds(at, q_block), left : left + LANES] = jnp.where(
                    half, one, two
                ).astype(BF16)
        return carry

    lax.fori_loop(0, count, block_step, 0)


def rope_table(rows, first_global):
    grid_rows = (rows + 2 * WINDOW) // GRID_W
    quarter = HEAD_DIM // 4
    freqs = ROPE_BASE ** (-jnp.arange(0, HEAD_DIM // 2, 2, dtype=F32) / (HEAD_DIM // 2))
    lane_freq = jnp.tile(freqs, LANES // quarter)
    row_at = (first_global - WINDOW) // GRID_W + jnp.arange(grid_rows, dtype=jnp.int32)
    spots = jnp.concatenate([row_at, jnp.arange(GRID_W, dtype=jnp.int32)]).astype(F32)
    angles = spots[:, None] * lane_freq[None, :]
    sign = jnp.where(jnp.arange(LANES) % (2 * quarter) < quarter, -1.0, 1.0)
    return jnp.concatenate([jnp.cos(angles), jnp.sin(angles) * sign[None, :]], axis=0)


def attention(q, k, v, left, right, sink, table, info, first, count, after):
    rows = q.shape[0]
    kv_width = k.shape[1]
    group = q.shape[1] // kv_width
    assert kv_width % LANES == 0 and group == 2 and rows % WINDOW == 0
    assert rows % GRID_W == 0 and WINDOW % GRID_W == 0
    q_block = WINDOW
    span = q_block + 2 * WINDOW
    heads = q.shape[1] // HEAD_DIM
    done = count * q_block
    return pl.pallas_call(
        functools.partial(attention_kernel, first, count),
        out_shape=jax.ShapeDtypeStruct((done, q.shape[1]), BF16),
        in_specs=[SMEM, SMEM, VMEM] + [HBM] * 3 + [VMEM] * 2 + [ANY],
        out_specs=VMEM,
        scratch_shapes=[
            pltpu.VMEM((done + 2 * WINDOW, kv_width), BF16),
            pltpu.VMEM((done + 2 * WINDOW, kv_width), BF16),
            pltpu.VMEM((q_block, span), F32),
            pltpu.VMEM((kv_width // LANES, 2 * group * q_block, span), F32),
            pltpu.VMEM((kv_width // LANES, 2 * group * q_block, span), BF16),
            pltpu.VMEM((done, q.shape[1]), BF16),
            pltpu.VMEM((done + 2 * WINDOW, kv_width), BF16),
            pltpu.SemaphoreType.DMA((3,)),
        ],
        cost_estimate=pl.CostEstimate(
            flops=24 * done * span * heads * HEAD_DIM,
            transcendentals=done * span * heads,
            bytes_accessed=8 * rows * kv_width * 2,
        ),
        compiler_params=params(16),
        name="attention",
    )(info, sink, table, q, k, v, left, right, after)


def mixer_kernel(rows_ref, weight_hbm, out_ref, weight_ref, total_ref, sems):
    parts, _, part = rows_ref.shape
    width = out_ref.shape[1]
    step = math.gcd(width, 512)
    spots = [slice(i * part, (i + 1) * part) for i in range(parts)]
    loads = [
        pltpu.make_async_copy(weight_hbm.at[spot, :], weight_ref.at[spot, :], sems.at[i])
        for i, spot in enumerate(spots)
    ]
    for load in loads:
        load.start()
    for i, spot in enumerate(spots):
        loads[i].wait()
        for left in range(0, width, step):
            cut = slice(left, left + step)
            total = jnp.dot(rows_ref[i], weight_ref[spot, cut], preferred_element_type=F32)
            if i:
                total = total + total_ref[:, cut]
            if i < parts - 1:
                total_ref[:, cut] = total
            else:
                out_ref[:, cut] = total.astype(BF16)


def mix(rows, weight):
    parts, tokens, _ = rows.shape
    width = weight.shape[1]
    return pl.pallas_call(
        mixer_kernel,
        out_shape=jax.ShapeDtypeStruct((tokens, width), BF16),
        in_specs=[VMEM, HBM],
        out_specs=VMEM,
        scratch_shapes=[
            pltpu.VMEM(weight.shape, BF16),
            pltpu.VMEM((tokens, width), F32),
            pltpu.SemaphoreType.DMA((parts,)),
        ],
        compiler_params=params(18),
        cost_estimate=cost(2e10),
        name="mixer",
    )(rows, pltpu.with_memory_space_constraint(weight, pltpu.HBM))


def relay(x, axis):
    return lax.ppermute(x, axis, [(0, 1), (1, 0)])


def layer(
    queries,
    key_heads,
    value_heads,
    sink_logits,
    mix_weight,
    expert_input,
    norm_gain,
    routes,
    route_weights,
    gate_weight,
    up_weight,
    down_weight,
):
    ring = ("zh", "zl", "xx")
    inner = ("xx", "tp")
    ring_size = lax.axis_size(ring)
    tp_size = lax.axis_size("tp")
    plane = lax.axis_size(inner)
    experts_all = ring_size * tp_size
    tok_local, top = routes.shape
    cap = 2 * tok_local * top // experts_all
    xor = plane <= 8 and plane & (plane - 1) == 0 and plane > 1

    def layout(i):
        if not xor:
            return 1, (top, cap, plane, 0)
        stride = STRIDE[i]
        return plane // stride, (top, cap, plane // stride, stride)

    position = lax.axis_index(inner)
    base = lax.axis_index(("zh", "zl")) * plane
    where = jnp.stack([base, position]).astype(jnp.int32)

    def mate(x, step):
        return lax.ppermute(x, inner, [(i, i ^ step) for i in range(plane)])

    def both(x, i):
        return [x, mate(x, 1)] if layout(i)[1][3] == 2 else [x]

    def exchange(parts, i):
        if not xor:
            block = parts[0].reshape(-1, plane, cap, parts[0].shape[1]).swapaxes(0, 1)
            turned = lax.all_to_all(block, inner, 0, 0, tiled=True)
            return [turned.swapaxes(0, 1).reshape(parts[0].shape)]
        stride = layout(i)[1][3]
        return [parts[0]] + [mate(parts[p], stride * p) for p in range(1, len(parts))]

    own = make_payload(expert_input, norm_gain, routes, route_weights)
    near = relay(own, "zl")
    far = relay(own, "zh")
    far_near = relay(far, "zl")

    rows_here = queries.shape[0]
    first_global = lax.axis_index(ring) * rows_here
    tail = jnp.concatenate([key_heads[-WINDOW:], value_heads[-WINDOW:]], axis=1)
    head = jnp.concatenate([key_heads[:WINDOW], value_heads[:WINDOW]], axis=1)
    ends = ring_size - 1
    left = lax.ppermute(tail, ring, [(i, i + 1) for i in range(ends)])
    right = lax.ppermute(head, ring, [(i + 1, i) for i in range(ends)])
    table = rope_table(rows_here, first_global)
    info = jnp.stack([first_global, jnp.int32(rows_here * ring_size)]).astype(jnp.int32)
    blocks = rows_here // WINDOW

    half = (blocks - 2) // 2
    ranges = ((1, half), (1 + half, blocks - 2 - half), (0, 1), (blocks - 1, 1))

    def attend(i, after):
        first, count = ranges[i]
        return attention(
            queries, key_heads, value_heads, left if i == 2 else table,
            right if i == 3 else table, sink_logits, table, info, first, count, after,
        )

    chunks = [both(x, i) for i, x in enumerate((own, near, far, far_near))]

    def send(i, after):
        pieces, plan = layout(i)
        parts = dispatch(plan, pieces, where, chunks[i], after)
        return exchange(parts, i), parts[0]

    held = [
        pltpu.with_memory_space_constraint(w, pltpu.VMEM)
        for w in (gate_weight, up_weight, down_weight)
    ]

    def work(i, after):
        return experts(arrived[i], held, after)

    arrived, made, rows = {}, {}, {}
    arrived[0], sent = send(0, [table, info])
    rows[0] = attend(0, sent)
    arrived[1], sent = send(1, [rows[0]])
    made[0] = work(0, [sent])
    arrived[2], sent = send(2, [made[0][0]])
    made[1] = work(1, [sent])
    arrived[3], sent = send(3, [made[1][0]])
    made[2] = work(2, [sent])
    made[3] = work(3, [made[2][0]])
    rows[3] = attend(3, made[3][0])
    rows[2] = attend(2, rows[3])
    rows[1] = attend(1, rows[2])
    attended = jnp.concatenate([rows[i] for i in (2, 0, 1, 3)], axis=0)

    back = {i: exchange(made[i], i) for i in (3, 2, 1, 0)}
    tp_blocks = attended.reshape(tp_size, rows_here // tp_size, attended.shape[1])
    token_rows = lax.all_to_all(tp_blocks, "tp", split_axis=0, concat_axis=0, tiled=True)

    def gather(i, after):
        own_part, *other = combine(layout(i)[1], where, chunks[i], back[i], after)
        return [own_part] + [mate(x, 1) for x in other], own_part

    parts, done = gather(1, [])
    side = add(parts) if len(parts) > 1 else parts[0].astype(BF16)
    parts, done = gather(3, [done])
    last = add(parts) if len(parts) > 1 else parts[0].astype(BF16)
    parts, done = gather(2, [last])
    mid = add(parts + [relay(last, "zl")])
    parts, _ = gather(0, [done])
    mixer_out = mix(token_rows, mix_weight)
    summed = add(parts + [relay(side, "zl"), relay(mid, "zh")])
    return (mixer_out, summed)


def solution(mesh):
    n_ep, n_tp = mesh.shape["ep"], mesh.shape["tp"]
    assert n_ep % 4 == 0
    fine = Mesh(mesh.devices.reshape(2, 2, n_ep // 4, n_tp), ("zh", "zl", "xx", "tp"))
    ring = ("zh", "zl", "xx")
    every = ring + ("tp",)
    return jax.shard_map(
        layer,
        mesh=fine,
        in_specs=(
            P(ring, "tp"),
            P(ring, "tp"),
            P(ring, "tp"),
            P("tp"),
            P(),
            P(every, None),
            P(),
            P(every, None),
            P(every, None),
            P(every, None, None),
            P(every, None, None),
            P(every, None, None),
        ),
        out_specs=(P(every, None), P(every, None)),
        check_vma=False,
    )
```
